32 devices in a mesh: grp: 2 (over x), sp: 4 (over y, core), tp: 4 (over z).
Axes of the slice: x: 2, y: 2, z: 4, core: 2. Of those that a mesh axis runs over, the one named last changes fastest.
Arguments:
- resid_in: bfloat16 [4096, 2048], P(('grp', 'sp', 'tp')), parts along dimension 0, may hold values from -6 to 6
- pool_input: bfloat16 [4096, 1024], P(('grp', 'sp'), 'tp'), parts along dimension 0, may hold values from -6 to 6
- pool_weight: bfloat16 [4, 256, 256], replicated, may hold values from -0.375 to 0.375
- pool_scale: float32 [1024], replicated, may hold values from 0.2 to 0.8
- out_weight: bfloat16 [1024, 2048], replicated, may hold values from -0.1875 to 0.1875
- mix_gain: float32 [2048], replicated, may hold values from 0.1 to 1.9
- ffn_gain: float32 [2048], replicated, may hold values from 0.1 to 1.9
- w_gate: bfloat16 [32, 2048, 1024], P('sp', None, 'tp'), may hold values from -0.375 to 0.375
- w_up: bfloat16 [32, 2048, 1024], P('sp', None, 'tp'), may hold values from -0.375 to 0.375
- w_down: bfloat16 [32, 1024, 2048], P('sp', 'tp'), may hold values from -0.1875 to 0.1875
- routes: int32 [4096, 2], P(('grp', 'sp', 'tp')), parts along dimension 0, may hold values from 0 to 31, all different within a row; in each aligned block of 128 rows (0 to 127, 128 to 255, ...) at most 9 rows name the same one
- route_weight: float32 [4096, 2], P(('grp', 'sp', 'tp')), parts along dimension 0, may hold values from 0.1 to 1
- post_gain: float32 [2048], replicated, may hold values from 0.1 to 1.9
Outputs:
- layer_out: bfloat16 [4096, 2048], P(('grp', 'sp', 'tp')), parts along dimension 0
The draws below stay inside these ranges and needn't reach their ends.
There are 2 independent parts, one for each index of `grp`. The reference program is written for one: setup_inputs(seed, part) draws one part's arguments, and reference() takes and returns one part's arrays. A program takes and returns all parts, laid end to end along the dimension named above; an argument that names none is the same for every part. Nothing has to cross between parts.
Inputs may be any that keep to these rules, and one draw needn't show every extreme that they name: `routes`: each row names 2 different experts. The rows of one device name any one expert at most 9 times, and in every draw some device's rows name some expert exactly 9 times.
All inputs are finite; a program needn't handle non-finite values.
Results may differ from the reference program's by a relative error of at most 0.011.
Values may be sent and summed in bfloat16 or wider, within the bound.
A program may use at most 128 MiB of HBM per device.

```python
import math
import jax
import jax.numpy as jnp
import numpy as np
from jax import lax

D = 2048
POOL_WIDTH = 1024
GROUPS = 4
GROUP_DIM = 256
FF = 1024
EXPERTS = 32
TOP = 2
TOK_DEV = 128
CAP = 9
SEQ = 2048
N_TP = 4


def shard_levels(key, shape, cuts, smallest, high):
    gain, own = 1.0, jax.random.fold_in(key, 6)
    for axis_at, shards_of in cuts:
        draws = jnp.exp(jax.random.uniform(jax.random.fold_in(own, axis_at), (shards_of,), jnp.float32, smallest / len(cuts), high / len(cuts)))
        gain = gain * jnp.repeat(draws, shape[axis_at] // shards_of).reshape([-1 if axis == axis_at else 1 for axis in range(len(shape))])
    return gain


def assign_block(own_key, own, number, rows, number_of, top, bound, skew):
    order = jax.random.permutation(own_key, number_of)
    packed, ordinary = shares(number_of, rows * top, bound, skew, True), shares(number_of, rows * top, bound, skew, False)
    places = jnp.arange(number_of)

    def named(sizes, offset_by):
        used = int((sizes > 0).sum())
        fixed = max(1, used // 4)
        passed = fixed + (places - fixed + offset_by * (used - fixed)) % max(1, number_of - fixed)
        return jnp.zeros((number_of,), jnp.int32).at[order[jnp.where(places < fixed, places, passed)]].set(jnp.asarray(sizes, jnp.int32))

    sizes = jnp.where(number % 4 == 0, named(packed, number // 4), named(ordinary, number - number // 4 - 1))
    mixed = jax.random.permutation(jax.random.fold_in(own, 3), number_of)
    source_of, sink = mixed[0:number_of // 2 * 2:2], mixed[1:number_of // 2 * 2:2]
    margin = jnp.minimum(sizes[source_of] - 1, bound - sizes[sink]) // 2
    margin = jnp.where((source_of == order[0]) | (sink == order[0]) | (sizes[sink] == 0), 0, jnp.maximum(margin, 0))
    passed = jax.random.randint(jax.random.fold_in(own, 4), (number_of // 2,), 0, 1 << 20) % (margin + 1)
    sizes = sizes.at[source_of].add(-passed).at[sink].add(passed)
    labels = jnp.searchsorted(jnp.cumsum(sizes), jnp.arange(rows * top), side="right").astype(jnp.int32)
    listing = labels.reshape(top, rows).T
    listing = listing[jax.random.permutation(jax.random.fold_in(own, 1), rows)]
    offset_by = jax.random.randint(jax.random.fold_in(own, 2), (rows, 1), 0, top)
    return jnp.take_along_axis(listing, (jnp.arange(top)[None, :] + offset_by) % top, axis=1)


def shares(count, total, limit, slope, full):
    portions = [(1 << 20) // math.isqrt(standing ** slope) + 1 for standing in range(1, count + 1)]
    largest = limit if full else min(limit, max(-(-total // count), total * portions[0] // sum(portions)))
    least = 1 if total - largest >= count - 1 else 0
    given, surplus = [largest] + [least] * (count - 1), total - largest - least * (count - 1)
    while surplus > 0:
        candidates = [i for i in range(1, count) if given[i] < largest] or [i for i in range(1, count) if given[i] < limit]
        pool, budget = sum([portions[i] for i in candidates]), surplus
        for i in candidates:
            more = min(limit - given[i], max(1, budget * portions[i] // pool), surplus)
            given[i] = given[i] + more
            surplus = surplus - more
    return np.array(given)


def gaussian(stream_key, extent, width, limit, split=(), kind=jnp.bfloat16):
    gain = shard_levels(stream_key, extent, split, -0.22, 0.18) if split else 1.0
    array = jax.random.normal(stream_key, extent, jnp.float32) * width * gain
    return jnp.minimum(jnp.maximum(array, -limit), limit).astype(kind)


def setup_inputs(seed: int = 0, part: int = 0) -> dict:
    seeds = jax.random.split(jax.random.key(seed), 14)
    own_keys = jax.random.split(jax.random.fold_in(seeds[13], part), 14)
    resid_in = gaussian(own_keys[0], (SEQ, D), 1.0, 6.0, ((0, 16),))
    pool_input = gaussian(own_keys[1], (SEQ, POOL_WIDTH), 1.0, 6.0, ((0, 4), (1, 4)))
    pool_weight = gaussian(seeds[2], (GROUPS, GROUP_DIM, GROUP_DIM), GROUP_DIM ** -0.5, 0.375)
    pool_scale = jnp.clip(jax.random.uniform(seeds[3], (POOL_WIDTH,), jnp.float32, 0.2, 0.8), 0.2, 0.8)
    out_weight = gaussian(seeds[4], (POOL_WIDTH, D), POOL_WIDTH ** -0.5, 0.1875)
    mix_gain = jnp.clip(1.0 + 0.18 * jax.random.normal(seeds[5], (D,), jnp.float32), 0.1, 1.9)
    ffn_gain = jnp.clip(1.0 + 0.18 * jax.random.normal(seeds[6], (D,), jnp.float32), 0.1, 1.9)
    w_gate = gaussian(seeds[7], (EXPERTS, D, FF), (D // 8) ** -0.5, 0.375, ((0, 4), (2, 4)))
    w_up = gaussian(seeds[8], (EXPERTS, D, FF), (D // 8) ** -0.5, 0.375, ((0, 4), (2, 4)))
    w_down = gaussian(seeds[9], (EXPERTS, FF, D), FF ** -0.5, 0.1875, ((0, 4), (1, 4)))
    routes_keys = jax.random.split(jax.random.fold_in(own_keys[10], 1), SEQ // TOK_DEV)
    routes_turns = jax.random.permutation(jax.random.fold_in(own_keys[10], 3), SEQ // TOK_DEV)
    routes = jax.vmap(lambda own, number: assign_block(jax.random.fold_in(own_keys[10], 2), own, number, TOK_DEV, EXPERTS, TOP, CAP, 1))(routes_keys, routes_turns).reshape((SEQ, TOP))
    route_weight = jnp.clip(jnp.exp(math.log(1.0) - 2.3025851 * jax.random.uniform(own_keys[11], (SEQ, TOP), jnp.float32) ** shard_levels(own_keys[11], (SEQ, TOP), ((0, 16),), -0.2, 0.2)), 0.1, 1.0)
    post_gain = jnp.clip(1.0 + 0.18 * jax.random.normal(seeds[12], (D,), jnp.float32), 0.1, 1.9)
    return {"resid_in": resid_in, "pool_input": pool_input, "pool_weight": pool_weight, "pool_scale": pool_scale, "out_weight": out_weight, "mix_gain": mix_gain, "ffn_gain": ffn_gain, "w_gate": w_gate, "w_up": w_up, "w_down": w_down, "routes": routes, "route_weight": route_weight, "post_gain": post_gain}


pool_windows = (2, 4, 8, 16)
reach_back = 15
norm_eps = 1e-06
clamp_limit = 7.0
glu_alpha = 1.702

def rms_scale(values, gain_vec):
    inverse = lax.rsqrt(lax.optimization_barrier(jnp.mean(values * values, axis=-1, keepdims=True)) + norm_eps)
    return values * inverse * gain_vec

def clamped_unit(gate_pre, upward):
    gate_clip = jnp.minimum(gate_pre, clamp_limit)
    linear = jnp.clip(upward, -clamp_limit, clamp_limit)
    return gate_clip * jax.nn.sigmoid(glu_alpha * gate_clip) * (linear + 1.0)

def reference(resid_in, pool_input, pool_weight, pool_scale, out_weight, mix_gain, ffn_gain, w_gate, w_up, w_down, routes, route_weight, post_gain):
    source = pool_input.astype(jnp.float32)
    positions = jnp.arange(SEQ, dtype=jnp.int32)
    pieces = []
    for group_level, win_len in enumerate(pool_windows):
        group_cols = source[:, group_level * GROUP_DIM:(group_level + 1) * GROUP_DIM]
        padded = jnp.concatenate([jnp.zeros((reach_back, GROUP_DIM), jnp.float32), group_cols], axis=0)
        running = jnp.zeros((SEQ, GROUP_DIM), jnp.float32)
        for offset in range(win_len):
            running = running + padded[reach_back - offset:reach_back - offset + SEQ]
        divisor = jnp.minimum(positions + 1, win_len).astype(jnp.float32)[:, None]
        pieces.append(running / divisor - group_cols)
    mixed_rows = jnp.concatenate(pieces, axis=1).astype(jnp.bfloat16)
    pooled = jnp.einsum('tgc,gcd->tgd', mixed_rows.reshape(SEQ, GROUPS, GROUP_DIM).astype(jnp.float32), pool_weight.astype(jnp.float32))
    pooled = (pooled * pool_scale.reshape(GROUPS, GROUP_DIM)).astype(jnp.bfloat16).reshape(SEQ, POOL_WIDTH)
    mix_out = jnp.dot(pooled, out_weight, preferred_element_type=jnp.float32)
    residual = (resid_in.astype(jnp.float32) + rms_scale(mix_out, mix_gain)).astype(jnp.bfloat16)
    normed = rms_scale(residual.astype(jnp.float32), ffn_gain).astype(jnp.bfloat16)
    flat_route = routes.reshape(-1).astype(jnp.int32)
    total = SEQ * TOP
    sort_order = jnp.argsort(flat_route, stable=True).astype(jnp.int32)
    token_of = (sort_order // TOP).astype(jnp.int32)
    counts = lax.optimization_barrier(jnp.sum((flat_route[:, None] == jnp.arange(EXPERTS, dtype=jnp.int32)[None, :]).astype(jnp.int32), axis=0))
    starts = (jnp.cumsum(counts) - counts).astype(jnp.int32)
    most_rows = SEQ // TOK_DEV * CAP
    block_ff = FF // N_TP

    def one_expert(expert):
        row_index = jnp.minimum(starts[expert] + jnp.arange(most_rows, dtype=jnp.int32), total - 1)
        taken_rows = normed[token_of[row_index]]
        gate_pre = jnp.dot(taken_rows, w_gate[expert], preferred_element_type=jnp.float32)
        upward = jnp.dot(taken_rows, w_up[expert], preferred_element_type=jnp.float32)
        activated = clamped_unit(gate_pre, upward).astype(jnp.bfloat16)
        partials = jnp.einsum('rnf,nfd->rnd', activated.reshape(most_rows, N_TP, block_ff).astype(jnp.float32), w_down[expert].reshape(N_TP, block_ff, D).astype(jnp.float32))
        partials = lax.optimization_barrier(partials.astype(jnp.bfloat16))
        return lax.optimization_barrier(jnp.sum(partials.astype(jnp.float32), axis=1)).astype(jnp.bfloat16)
    expert_outs = lax.map(one_expert, jnp.arange(EXPERTS, dtype=jnp.int32))
    sorted_e = flat_route[sort_order]
    local_pos = (jnp.arange(total, dtype=jnp.int32) - starts[sorted_e]).astype(jnp.int32)
    picked = expert_outs[sorted_e, local_pos]
    assigned = jnp.zeros((total, D), jnp.bfloat16).at[sort_order].set(picked)
    expert_mix = lax.optimization_barrier(jnp.sum(assigned.reshape(SEQ, TOP, D).astype(jnp.float32) * route_weight[:, :, None], axis=1))
    return (residual.astype(jnp.float32) + rms_scale(expert_mix, post_gain)).astype(jnp.bfloat16)
```

```python
import functools

import jax
import jax.numpy as jnp
from jax import lax
from jax.experimental import pallas as pl
from jax.experimental.pallas import tpu as pltpu
from jax.sharding import PartitionSpec as P

GROUPS = 4
GROUP_DIM = 256
TOP = 2
CAP = 9


pool_windows = (2, 4, 8, 16)
reach_back = 15
norm_eps = 1e-06
clamp_limit = 7.0
glu_alpha = 1.702


def passed_along(x, axis, by):
    size = lax.axis_size(axis)
    pairs = [(i, i + by) for i in range(size) if 0 <= i + by < size]
    return lax.ppermute(x, axis, pairs)


def rms_scale(values, gain_vec):
    inverse = lax.rsqrt(jnp.mean(values * values, axis=-1, keepdims=True) + norm_eps)
    return values * inverse * gain_vec


def clamped_unit(gate_pre, upward):
    gate_clip = jnp.minimum(gate_pre, clamp_limit)
    linear = jnp.clip(upward, -clamp_limit, clamp_limit)
    return gate_clip * jax.nn.sigmoid(glu_alpha * gate_clip) * (linear + 1.0)


SLOT = 16
Y_FIRST = 48
MESH = pl.DeviceIdType.MESH


def coords():
    return lax.axis_index("grp"), lax.axis_index("sp"), lax.axis_index("tp")


def line_barrier(n_tp, others):
    grp, sp, tp = coords()
    barrier = pltpu.get_barrier_semaphore()
    for by in others:
        target = (grp, (sp + by[0]) % 4, (tp + by[1]) % n_tp)
        pl.semaphore_signal(barrier, inc=1, device_id=target, device_id_type=MESH)
    pl.semaphore_wait(barrier, len(others))


def gather_kernel(n_tp, cuts, row_ref, meta_ref, all_ref, all_meta, send, recv, msend, mrecv, own):
    grp, sp, tp = coords()
    yy, core = sp // 2, sp % 2
    y_other = (1 - yy) * 2 + core
    c_other = yy * 2 + (1 - core)
    others = [(a, b) for a in range(4) for b in range(n_tp) if (a, b) != (0, 0)]
    own_copy = pltpu.make_async_copy(row_ref, all_ref.at[sp, tp], own.at[0])
    own_copy.start()
    own_meta = pltpu.make_async_copy(meta_ref, all_meta.at[sp, tp], own.at[1])
    own_meta.start()
    line_barrier(n_tp, others)

    def meta_copy(number, by):
        return pltpu.make_async_remote_copy(
            src_ref=meta_ref, dst_ref=all_meta.at[sp, tp],
            send_sem=msend.at[number], recv_sem=mrecv.at[number],
            device_id=(grp, (sp + by[0]) % 4, (tp + by[1]) % n_tp), device_id_type=MESH)

    own_copy.wait()
    own_meta.wait()

    def copy(s, t, part, way):
        target = [(grp, sp, tp + 1), (grp, sp, tp - 1), (grp, y_other, tp), (grp, c_other, tp)][way]
        first, count = cuts[part]
        piece = all_ref.at[s, t, pl.ds(first, count)]
        return pltpu.make_async_remote_copy(
            src_ref=piece, dst_ref=piece,
            send_sem=send.at[s, t, part, way], recv_sem=recv.at[s, t, part],
            device_id=target, device_id_type=MESH)

    def arrived(s, t, part):
        copy(s, t, part, 3).wait_recv()

    def guarded(cond, what):
        pl.when(cond)(what)

    sent = []

    def push(cond, s, t, part, way):
        if way == 0:
            cond = jnp.logical_and(cond, tp + 1 < n_tp)
        if way == 1:
            cond = jnp.logical_and(cond, tp > 0)
        guarded(cond, lambda: copy(s, t, part, way).start())
        sent.append((cond, s, t, part, way))

    yes = tp >= 0
    push(yes, sp, tp, 0, 2)
    push(yes, sp, tp, 1, 0)
    push(yes, sp, tp, 1, 1)
    push(yes, sp, tp, 1, 2)
    push(yes, sp, tp, 0, 0)
    push(yes, sp, tp, 0, 1)
    push(yes, sp, tp, 0, 3)
    push(yes, sp, tp, 1, 3)
    for number, by in enumerate(others):
        meta_copy(number, by).start()
    arrived(y_other, tp, 0)
    push(yes, y_other, tp, 0, 0)
    push(yes, y_other, tp, 0, 1)
    push(yes, y_other, tp, 0, 3)
    for dist in range(1, n_tp):
        for s, part in ((sp, 1), (sp, 0), (y_other, 0)):
            for way in (0, 1):
                t = tp - dist if way == 0 else tp + dist
                cond = t >= 0 if way == 0 else t < n_tp
                guarded(cond, functools.partial(arrived, s, t, part))
                push(cond, s, t, part, way)
                if part == 1:
                    push(cond, s, t, part, 2)
                push(cond, s, t, part, 3)
        for t, cond in (((tp, yes),) if dist == 1 else ()):
            arrived(y_other, t, 1)
            push(yes, y_other, t, 1, 3)
    for dist in range(1, n_tp):
        for way in (0, 1):
            t = tp - dist if way == 0 else tp + dist
            cond = t >= 0 if way == 0 else t < n_tp
            guarded(cond, functools.partial(arrived, y_other, t, 1))
            push(cond, y_other, t, 1, 3)
    cross = (yes, c_other), (yes, (1 - yy) * 2 + (1 - core))
    for _, s in cross:
        for t in range(n_tp):
            for part in (0, 1):
                arrived(s, t, part)
    for cond, s, t, part, way in sent:
        guarded(cond, lambda s=s, t=t, part=part, way=way: copy(s, t, part, way).wait_send())
    for number, by in enumerate(others):
        meta_copy(number, by).wait()


def gather_all(normed, meta, n_tp):
    tok, width = normed.shape
    first = min(Y_FIRST, tok // 2)
    cuts = ((0, first), (first, tok - first))
    vmem = pl.BlockSpec(memory_space=pltpu.VMEM)
    return pl.pallas_call(
        functools.partial(gather_kernel, n_tp, cuts),
        out_shape=(
            jax.ShapeDtypeStruct((4, n_tp, tok, width), normed.dtype),
            jax.ShapeDtypeStruct((4, n_tp) + meta.shape, meta.dtype),
        ),
        in_specs=[vmem, vmem],
        out_specs=(vmem, vmem),
        scratch_shapes=[
            pltpu.SemaphoreType.DMA((4, n_tp, 2, 4)),
            pltpu.SemaphoreType.DMA((4, n_tp, 2)),
            pltpu.SemaphoreType.DMA((4 * n_tp - 1,)),
            pltpu.SemaphoreType.DMA((4 * n_tp - 1,)),
            pltpu.SemaphoreType.DMA((2,)),
        ],
        compiler_params=pltpu.CompilerParams(
            collective_id=0, has_side_effects=True, vmem_limit_bytes=40 * 2**20
        ),
        name="gather_rows",
    )(normed, meta)


def add_into(dst, src):
    rows = dst.shape[0]
    strip = 16

    def body(i, carry):
        at = pl.ds(pl.multiple_of(i * strip, strip), strip)
        dst[at] = (dst[at].astype(jnp.float32) + src[at].astype(jnp.float32)).astype(dst.dtype)
        return carry

    lax.fori_loop(0, rows // strip, body, 0)


def scatter_kernel(n_tp, cuts, part_ref, out_ref, work, from_core, za, zb, ya, yb,
                   csend, crecv, asend, arecv, bsend, brecv, ysend, yrecv, own):
    grp, sp, tp = coords()
    yy, core = sp // 2, sp % 2
    yo = 1 - yy
    y_other = yo * 2 + core
    c_other = yy * 2 + (1 - core)
    nears = [(grp, y_other, tp), (grp, c_other, tp)]
    barrier = pltpu.get_barrier_semaphore()
    for target in nears:
        pl.semaphore_signal(barrier, inc=1, device_id=target, device_id_type=MESH)
    up_ok, down_ok = tp + 1 < n_tp, tp > 0
    ups, downs = (grp, sp, tp + 1), (grp, sp, tp - 1)
    for ok, target in ((up_ok, ups), (down_ok, downs)):
        pl.when(ok)(lambda target=target: pl.semaphore_signal(
            barrier, inc=1, device_id=target, device_id_type=MESH))
    pl.semaphore_wait(barrier, 2 + up_ok.astype(jnp.int32) + down_ok.astype(jnp.int32))
    (a0, an), (b0, bn) = cuts
    rows_a, rows_b = pl.ds(a0, an), pl.ds(b0, bn)

    def remote(src, dst, s_sem, r_sem, target):
        return pltpu.make_async_remote_copy(
            src_ref=src, dst_ref=dst, send_sem=s_sem, recv_sem=r_sem,
            device_id=target, device_id_type=MESH)

    def core_copy(y, t):
        return remote(part_ref.at[y * 2 + (1 - core), t], from_core.at[y, t],
                      csend.at[y, t], crecv.at[y, t], (grp, c_other, tp))

    order = []
    for dist in range(n_tp - 1, -1, -1):
        for side in (1, -1) if dist else (1,):
            t = tp + side * dist
            order.append((jnp.logical_and(t >= 0, t < n_tp), t, side, dist))
    for y in (yo, yy):
        for ok, t, side, dist in order:
            pl.when(ok)(lambda y=y, t=t: core_copy(y, t).start())
    for y in (0, 1):
        for t in range(n_tp):
            pltpu.make_async_copy(part_ref.at[y * 2 + core, t], work.at[y, t], own.at[y, t]).start()

    def y_copy_b(t):
        return remote(work.at[yo, t, rows_b], yb.at[t], ysend.at[t], yrecv.at[t], (grp, y_other, tp))

    def y_copy_a():
        return remote(work.at[yo, tp, rows_a], ya, ysend.at[n_tp], yrecv.at[n_tp], (grp, y_other, tp))

    def local(y, t):
        pltpu.make_async_copy(part_ref.at[y * 2 + core, t], work.at[y, t], own.at[y, t]).wait()
        core_copy(y, t).wait_recv()
        add_into(work.at[y, t], from_core.at[y, t])

    def z_copy(part, y, t, side):
        buf, ss, rs, rows = ((za, asend, arecv, rows_a), (zb, bsend, brecv, rows_b))[part]
        if side == 1:
            slot, target = t, ups
        else:
            slot = jnp.where(t == tp - 1, n_tp, t)
            target = downs
        row = y if part == 0 else 0
        return remote(work.at[y, t, rows], buf.at[row, slot], ss.at[row, t], rs.at[row, slot], target)

    def take_z(part, y, t, slot):
        buf, ss, rs, rows = ((za, asend, arecv, rows_a), (zb, bsend, brecv, rows_b))[part]
        row = y if part == 0 else 0
        remote(work.at[y, t, rows], buf.at[row, slot], ss.at[row, t], rs.at[row, slot], ups).wait_recv()
        add_into(work.at[y, t, rows], buf.at[row, slot])

    def z_step(part, y, t, side):
        inner = tp > 0 if side == 1 else tp + 1 < n_tp
        pl.when(inner)(lambda: take_z(part, y, t, t))
        z_copy(part, y, t, side).start()

    def z_end(part, y):
        pl.when(down_ok)(lambda: take_z(part, y, tp, tp))
        pl.when(up_ok)(lambda: take_z(part, y, tp, n_tp))

    for ok, t, side, dist in order:
        @pl.when(ok)
        def _(t=t):
            local(yo, t)
            y_copy_b(t).start()
    for ok, t, side, dist in order:
        @pl.when(ok)
        def _(t=t, side=side, dist=dist):
            local(yy, t)
            if dist:
                z_step(0, yo, t, side)
                z_step(0, yy, t, side)
            y_copy_b(t).wait_recv()
            add_into(work.at[yy, t, rows_b], yb.at[t])
            if dist:
                z_step(1, yy, t, side)
    z_end(0, yo)
    y_copy_a().start()
    z_end(0, yy)
    z_end(1, yy)
    y_copy_a().wait_recv()
    add_into(work.at[yy, tp, rows_a], ya)
    last = pltpu.make_async_copy(work.at[yy, tp], out_ref, own.at[0, 0])
    last.start()
    last.wait()
    y_copy_a().wait_send()
    for ok, t, side, dist in order:
        @pl.when(ok)
        def _(t=t, side=side, dist=dist):
            core_copy(yo, t).wait_send()
            core_copy(yy, t).wait_send()
            y_copy_b(t).wait_send()
            if dist:
                z_copy(0, yo, t, side).wait_send()
                z_copy(0, yy, t, side).wait_send()
                z_copy(1, yy, t, side).wait_send()


def scatter_sums(parts, n_tp):
    tok, width = parts.shape[2:]
    first = min(Y_FIRST, tok // 2)
    cuts = ((0, first), (first, tok - first))
    an, bn = cuts[0][1], cuts[1][1]
    vmem = pl.BlockSpec(memory_space=pltpu.VMEM)
    kind = parts.dtype
    return pl.pallas_call(
        functools.partial(scatter_kernel, n_tp, cuts),
        out_shape=jax.ShapeDtypeStruct((tok, width), kind),
        in_specs=[vmem],
        out_specs=vmem,
        scratch_shapes=[
            pltpu.VMEM((2, n_tp, tok, width), kind),
            pltpu.VMEM((2, n_tp, tok, width), kind),
            pltpu.VMEM((2, n_tp + 1, an, width), kind),
            pltpu.VMEM((1, n_tp + 1, bn, width), kind),
            pltpu.VMEM((an, width), kind),
            pltpu.VMEM((n_tp, bn, width), kind),
            pltpu.SemaphoreType.DMA((2, n_tp)),
            pltpu.SemaphoreType.DMA((2, n_tp)),
            pltpu.SemaphoreType.DMA((2, n_tp)),
            pltpu.SemaphoreType.DMA((2, n_tp + 1)),
            pltpu.SemaphoreType.DMA((1, n_tp)),
            pltpu.SemaphoreType.DMA((1, n_tp + 1)),
            pltpu.SemaphoreType.DMA((n_tp + 1,)),
            pltpu.SemaphoreType.DMA((n_tp + 1,)),
            pltpu.SemaphoreType.DMA((2, n_tp)),
        ],
        compiler_params=pltpu.CompilerParams(
            collective_id=1, has_side_effects=True, vmem_limit_bytes=48 * 2**20
        ),
        name="scatter_sums",
    )(parts)


def dense_experts(normed, routes, route_weight, w_gate, w_up, w_down):
    n_sp, n_tp = lax.axis_size("sp"), lax.axis_size("tp")
    tok, width = normed.shape
    local_experts = w_gate.shape[0]
    n_experts = local_experts * n_sp
    flat_route = routes.reshape(-1)
    onehot = (flat_route[:, None] == lax.iota(jnp.int32, n_experts)[None, :]).astype(jnp.int32)
    rank = jnp.sum((jnp.cumsum(onehot, axis=0) - onehot) * onehot, axis=1).reshape(tok, TOP)
    place = (routes * SLOT + rank).astype(jnp.float32)
    meta = jnp.concatenate([place, route_weight, jnp.zeros((tok, 8 - 2 * TOP), jnp.float32)], axis=1).T
    rows, metas = gather_all(normed, meta, n_tp)
    sources = n_sp * n_tp
    rows = rows.reshape(sources, tok, width)
    metas = metas.reshape(sources, 8, tok)
    slots = local_experts * SLOT
    index = metas[:, :TOP].astype(jnp.int32) - lax.axis_index("sp") * slots
    hit = index[:, :, None, :] == lax.iota(jnp.int32, slots)[None, None, :, None]
    weight = jnp.sum(jnp.where(hit, metas[:, TOP : 2 * TOP, None, :], 0.0), axis=(1, 3))
    pick = jnp.any(hit, axis=1).astype(jnp.bfloat16)
    held = jnp.einsum("sct,std->scd", pick, rows, preferred_element_type=jnp.float32)
    held = held.astype(jnp.bfloat16).reshape(sources, local_experts, SLOT, width)
    held = held.transpose(1, 0, 2, 3).reshape(local_experts, sources * SLOT, width)
    gate_pre = jnp.einsum("erd,edf->erf", held, w_gate, preferred_element_type=jnp.float32)
    upward = jnp.einsum("erd,edf->erf", held, w_up, preferred_element_type=jnp.float32)
    weight = weight.reshape(sources, local_experts, SLOT).transpose(1, 0, 2)
    activated = clamped_unit(gate_pre, upward) * weight.reshape(local_experts, sources * SLOT, 1)
    activated = activated.astype(jnp.bfloat16)
    terms = jnp.einsum("erf,efd->erd", activated, w_down, preferred_element_type=jnp.float32)
    terms = terms.astype(jnp.bfloat16).reshape(local_experts, sources, SLOT, width)
    terms = terms.transpose(1, 0, 2, 3).reshape(sources, slots, width)
    sums = jnp.einsum("sct,scd->std", pick, terms, preferred_element_type=jnp.float32)
    sums = sums.astype(jnp.bfloat16).reshape(n_sp, n_tp, tok, width)
    return scatter_sums(sums, n_tp).astype(jnp.float32)


def per_device(
    resid_in,
    pool_input,
    pool_weight,
    pool_scale,
    out_weight,
    mix_gain,
    ffn_gain,
    w_gate,
    w_up,
    w_down,
    routes,
    route_weight,
    post_gain,
):
    n_sp = lax.axis_size("sp")
    n_tp = lax.axis_size("tp")
    seg_rows, channels = pool_input.shape
    last_rows = pool_input[seg_rows - reach_back :]
    before = passed_along(last_rows, "sp", 1)
    extended = jnp.concatenate([before, pool_input], axis=0).astype(jnp.float32)
    first_chan = lax.axis_index("tp") * channels
    chan_group = (first_chan + lax.iota(jnp.int32, channels)) // GROUP_DIM
    positions = lax.axis_index("sp") * seg_rows + lax.iota(jnp.int32, seg_rows)
    window = jnp.zeros((channels,), jnp.int32)
    for group_level, win_len in enumerate(pool_windows):
        window = jnp.where(chan_group == group_level, win_len, window)
    running = jnp.zeros((seg_rows, channels), jnp.float32)
    window_sum = running
    for offset in range(pool_windows[-1]):
        running = running + extended[reach_back - offset : reach_back - offset + seg_rows]
        if offset + 1 in pool_windows:
            window_sum = jnp.where(window[None, :] == offset + 1, running, window_sum)
    divisor = jnp.minimum(positions[:, None] + 1, window[None, :]).astype(jnp.float32)
    mixed_rows = (window_sum / divisor - extended[reach_back:]).astype(jnp.bfloat16)
    token_mixed = lax.all_to_all(mixed_rows, "tp", split_axis=0, concat_axis=1, tiled=True)
    tok_rows = token_mixed.shape[0]
    pooled = jnp.einsum(
        "tgc,gcd->tgd",
        token_mixed.reshape(tok_rows, GROUPS, GROUP_DIM),
        pool_weight,
        preferred_element_type=jnp.float32,
    )
    pooled = (
        (pooled * pool_scale.reshape(GROUPS, GROUP_DIM)).astype(jnp.bfloat16).reshape(tok_rows, -1)
    )
    mix_out = jnp.dot(pooled, out_weight, preferred_element_type=jnp.float32)
    residual = (resid_in.astype(jnp.float32) + rms_scale(mix_out, mix_gain)).astype(jnp.bfloat16)
    normed = rms_scale(residual.astype(jnp.float32), ffn_gain).astype(jnp.bfloat16)
    width = normed.shape[1]
    if n_sp == 4 and n_tp <= 4 and tok_rows % 32 == 0 and tok_rows * width <= 128 * 2048:
        expert_mix = dense_experts(normed, routes, route_weight, w_gate, w_up, w_down)
        return (residual.astype(jnp.float32) + rms_scale(expert_mix, post_gain)).astype(jnp.bfloat16)
    local_experts = w_gate.shape[0]
    n_experts = local_experts * n_sp
    slot_total = n_experts * CAP
    flat_route = routes.reshape(-1)
    onehot = (flat_route[:, None] == lax.iota(jnp.int32, n_experts)[None, :]).astype(jnp.int32)
    slot_rank = jnp.sum((jnp.cumsum(onehot, axis=0) - onehot) * onehot, axis=1)
    slot_index = flat_route * CAP + slot_rank
    picker = slot_index[:, None] == lax.iota(jnp.int32, slot_total)[None, :]
    picker_rows = picker.astype(jnp.bfloat16)
    token_pick = jnp.sum(
        picker.reshape(tok_rows, TOP, slot_total).astype(jnp.float32), axis=1
    ).astype(jnp.bfloat16)
    buffer = lax.dot_general(
        token_pick, normed, (((0,), (0,)), ((), ())), preferred_element_type=jnp.float32
    )
    outgoing = buffer.astype(jnp.bfloat16).reshape(n_sp, local_experts * CAP, width)
    at_owner = lax.all_to_all(outgoing, "sp", split_axis=0, concat_axis=0, tiled=True)
    arrived = lax.all_gather(at_owner[:, None], "tp", axis=1, tiled=True)
    arrived = arrived.reshape(n_sp, n_tp, local_experts, CAP, width)
    gate_pre = jnp.einsum("sklcd,ldf->sklcf", arrived, w_gate, preferred_element_type=jnp.float32)
    upward = jnp.einsum("sklcd,ldf->sklcf", arrived, w_up, preferred_element_type=jnp.float32)
    activated = clamped_unit(gate_pre, upward).astype(jnp.bfloat16)
    terms = jnp.einsum("sklcf,lfd->kslcd", activated, w_down, preferred_element_type=jnp.float32)
    summed = lax.psum_scatter(
        terms.reshape(1 * lax.axis_size("tp"), n_sp, local_experts * CAP, width).astype(
            jnp.bfloat16
        ),
        "tp",
        scatter_dimension=0,
        tiled=True,
    ).astype(jnp.float32)
    results = summed[0].astype(jnp.bfloat16)
    returned = lax.all_to_all(results, "sp", split_axis=0, concat_axis=0, tiled=True).reshape(
        slot_total, width
    )
    gathered = jnp.dot(picker_rows, returned, preferred_element_type=jnp.float32)
    expert_mix = jnp.sum(gathered.reshape(tok_rows, TOP, width) * route_weight[:, :, None], axis=1)
    return (residual.astype(jnp.float32) + rms_scale(expert_mix, post_gain)).astype(jnp.bfloat16)


def solution(mesh):
    in_specs = (
        P(("grp", "sp", "tp"), None),
        P(("grp", "sp"), "tp"),
        P(),
        P(),
        P(),
        P(),
        P(),
        P("sp", None, "tp"),
        P("sp", None, "tp"),
        P("sp", "tp", None),
        P(("grp", "sp", "tp"), None),
        P(("grp", "sp", "tp"), None),
        P(),
    )
    out_specs = P(("grp", "sp", "tp"), None)
    return jax.shard_map(
        per_device, mesh=mesh, in_specs=in_specs, out_specs=out_specs, check_vma=False
    )
```

```python
import functools

import jax
import jax.numpy as jnp
from jax import lax
from jax.experimental import pallas as pl
from jax.experimental.pallas import tpu as pltpu
from jax.sharding import PartitionSpec as P

GROUPS = 4
GROUP_DIM = 256
TOP = 2
CAP = 9


pool_windows = (2, 4, 8, 16)
reach_back = 15
norm_eps = 1e-06
clamp_limit = 7.0
glu_alpha = 1.702


def passed_along(x, axis, by):
    size = lax.axis_size(axis)
    pairs = [(i, i + by) for i in range(size) if 0 <= i + by < size]
    return lax.ppermute(x, axis, pairs)


def rms_scale(values, gain_vec):
    inverse = lax.rsqrt(jnp.mean(values * values, axis=-1, keepdims=True) + norm_eps)
    return values * inverse * gain_vec


def clamped_unit(gate_pre, upward):
    gate_clip = jnp.minimum(gate_pre, clamp_limit)
    linear = jnp.clip(upward, -clamp_limit, clamp_limit)
    return gate_clip * jax.nn.sigmoid(glu_alpha * gate_clip) * (linear + 1.0)


SLOT = 16
Y_FIRST = 16
MESH = pl.DeviceIdType.MESH


def coords():
    return lax.axis_index("grp"), lax.axis_index("sp"), lax.axis_index("tp")


def layer_kernel(n_tp, cuts, row_ref, meta_ref, wg_ref, wu_ref, wd_ref, out_ref,
                 every, metas, picks, weights, held, wg, wu, wd,
                 work, from_core, za, zb, ya, yb,
                 send, recv, msend, mrecv, wsem,
                 csend, crecv, asend, arecv, bsend, brecv, ysend, yrecv, own):
    grp, sp, tp = coords()
    yy, core = sp // 2, sp % 2
    yo = 1 - yy
    y_other = yo * 2 + core
    c_other = yy * 2 + (1 - core)
    tok, width = row_ref.shape
    local_experts, buffers = wg_ref.shape[0], wg.shape[0]
    slots = local_experts * SLOT
    chunk = min(512, width)
    others = [(a, b) for a in range(4) for b in range(n_tp) if (a, b) != (0, 0)]

    def weight_copies(e):
        at = lax.rem(e, buffers)
        return [pltpu.make_async_copy(w.at[e], buf.at[at], wsem.at[i, at])
                for i, (w, buf) in enumerate(((wg_ref, wg), (wu_ref, wu), (wd_ref, wd)))]

    own_copy = pltpu.make_async_copy(row_ref, every.at[sp, tp], own.at[0, 0])
    own_copy.start()
    own_meta = pltpu.make_async_copy(meta_ref, metas.at[sp, tp], own.at[0, 1])
    own_meta.start()
    barrier = pltpu.get_barrier_semaphore()
    for by in others:
        target = (grp, (sp + by[0]) % 4, (tp + by[1]) % n_tp)
        pl.semaphore_signal(barrier, inc=1, device_id=target, device_id_type=MESH)
    pl.semaphore_wait(barrier, len(others))

    def meta_copy(number, by):
        return pltpu.make_async_remote_copy(
            src_ref=meta_ref, dst_ref=metas.at[sp, tp],
            send_sem=msend.at[number], recv_sem=mrecv.at[number],
            device_id=(grp, (sp + by[0]) % 4, (tp + by[1]) % n_tp), device_id_type=MESH)

    own_copy.wait()
    own_meta.wait()

    def copy(s, t, part, way):
        target = [(grp, sp, tp + 1), (grp, sp, tp - 1), (grp, y_other, tp), (grp, c_other, tp)][way]
        first, count = cuts[part]
        piece = every.at[s, t, pl.ds(first, count)]
        return pltpu.make_async_remote_copy(
            src_ref=piece, dst_ref=piece,
            send_sem=send.at[s, t, part, way], recv_sem=recv.at[s, t, part],
            device_id=target, device_id_type=MESH)

    def arrived(s, t, part):
        copy(s, t, part, 3).wait_recv()

    sent = []

    def push(cond, s, t, part, way):
        if way == 0:
            cond = jnp.logical_and(cond, tp + 1 < n_tp)
        if way == 1:
            cond = jnp.logical_and(cond, tp > 0)
        pl.when(cond)(lambda: copy(s, t, part, way).start())
        sent.append((cond, s, t, part, way))

    def source_rows(s, t):
        return pl.ds(pl.multiple_of((s * n_tp + t) * SLOT, SLOT), SLOT)

    def select(s, t):
        slot = lax.broadcasted_iota(jnp.int32, (slots, tok), 0).astype(jnp.float32)
        base = (sp * slots).astype(jnp.float32)
        meta = metas[s, t]
        pick = jnp.zeros((slots, tok), jnp.float32)
        weight = jnp.zeros((slots, tok), jnp.float32)
        for k in range(TOP):
            hit = (meta[k : k + 1] - base) == slot
            pick = pick + jnp.where(hit, 1.0, 0.0)
            weight = weight + jnp.where(hit, meta[TOP + k : TOP + k + 1], 0.0)
        weight = jnp.broadcast_to(jnp.sum(weight, axis=1, keepdims=True), (slots, 128))
        pick = pick.astype(jnp.bfloat16)
        picks[s, t] = pick
        for e in range(local_experts):
            weights[e, source_rows(s, t)] = weight[e * SLOT : (e + 1) * SLOT]

        def body(i, carry):
            at = pl.ds(pl.multiple_of(i * chunk, chunk), chunk)
            got = jnp.dot(pick, every[s, t, :, at], preferred_element_type=jnp.float32)
            got = got.astype(jnp.bfloat16)
            for e in range(local_experts):
                held[e, source_rows(s, t), at] = got[e * SLOT : (e + 1) * SLOT]
            return carry

        lax.fori_loop(0, width // chunk, body, 0)

    yes = tp >= 0
    for number, by in enumerate(others):
        meta_copy(number, by).start()
    push(yes, sp, tp, 0, 2)
    push(yes, sp, tp, 1, 0)
    push(yes, sp, tp, 1, 1)
    push(yes, sp, tp, 1, 2)
    push(yes, sp, tp, 0, 0)
    push(yes, sp, tp, 0, 1)
    push(yes, sp, tp, 0, 3)
    push(yes, sp, tp, 1, 3)
    for e in range(min(buffers, local_experts)):
        for c in weight_copies(e):
            c.start()
    arrived(y_other, tp, 0)
    push(yes, y_other, tp, 0, 0)
    push(yes, y_other, tp, 0, 1)
    push(yes, y_other, tp, 0, 3)
    select(sp, tp)
    for number, by in enumerate(others):
        meta_copy(number, by).wait()
    for dist in range(1, n_tp):
        for s, part in ((sp, 1), (sp, 0), (y_other, 0)):
            for way in (0, 1):
                t = tp - dist if way == 0 else tp + dist
                cond = t >= 0 if way == 0 else t < n_tp
                pl.when(cond)(functools.partial(arrived, s, t, part))
                push(cond, s, t, part, way)
                if part == 1:
                    push(cond, s, t, part, 2)
                push(cond, s, t, part, 3)
        if dist == 1:
            arrived(y_other, tp, 1)
            push(yes, y_other, tp, 1, 3)
            select(y_other, tp)
        for way in (0, 1):
            t = tp - dist if way == 0 else tp + dist
            cond = t >= 0 if way == 0 else t < n_tp
            pl.when(cond)(functools.partial(select, sp, t))
    for dist in range(1, n_tp):
        for way in (0, 1):
            t = tp - dist if way == 0 else tp + dist
            cond = t >= 0 if way == 0 else t < n_tp
            pl.when(cond)(functools.partial(arrived, y_other, t, 1))
            push(cond, y_other, t, 1, 3)
            pl.when(cond)(functools.partial(select, y_other, t))
    for s in (c_other, yo * 2 + (1 - core)):
        def cross(t, carry, s=s):
            for part in (0, 1):
                arrived(s, t, part)
            select(s, t)
            return carry

        lax.fori_loop(0, n_tp, cross, 0)
    for cond, s, t, part, way in sent:
        pl.when(cond)(lambda s=s, t=t, part=part, way=way: copy(s, t, part, way).wait_send())

    def expert(e, carry):
        at = lax.rem(e, buffers)
        for c in weight_copies(e):
            c.wait()
        rows = held[e]
        gate_pre = jnp.dot(rows, wg[at], preferred_element_type=jnp.float32)
        upward = jnp.dot(rows, wu[at], preferred_element_type=jnp.float32)
        scale = jnp.concatenate([weights[e]] * (gate_pre.shape[1] // 128), axis=1)
        activated = (clamped_unit(gate_pre, upward) * scale).astype(jnp.bfloat16)

        def down(i, inner):
            cols = pl.ds(pl.multiple_of(i * chunk, chunk), chunk)
            term = jnp.dot(activated, wd[at, :, cols], preferred_element_type=jnp.float32)
            held[e, :, cols] = term.astype(jnp.bfloat16)
            return inner

        lax.fori_loop(0, width // chunk, down, 0)

        @pl.when(e + buffers < local_experts)
        def _():
            for c in weight_copies(e + buffers):
                c.start()

        return carry

    lax.fori_loop(0, local_experts, expert, 0)

    def combined(s, t, at):
        term = held[:, source_rows(s, t), at].reshape(slots, chunk)
        return lax.dot_general(picks[s, t], term, (((0,), (0,)), ((), ())),
                               preferred_element_type=jnp.float32)

    (a0, an), (b0, bn) = cuts
    rows_a, rows_b = pl.ds(a0, an), pl.ds(b0, bn)
    ups, downs = (grp, sp, tp + 1), (grp, sp, tp - 1)
    up_ok, down_ok = tp + 1 < n_tp, tp > 0

    def remote(src, dst, s_sem, r_sem, target):
        return pltpu.make_async_remote_copy(
            src_ref=src, dst_ref=dst, send_sem=s_sem, recv_sem=r_sem,
            device_id=target, device_id_type=MESH)

    def core_copy(y, t):
        return remote(every.at[y * 2 + (1 - core), t], from_core.at[y, t],
                      csend.at[y, t], crecv.at[y, t], (grp, c_other, tp))

    def combine_away(y, t):
        s = y * 2 + (1 - core)

        def body(i, carry):
            at = pl.ds(pl.multiple_of(i * chunk, chunk), chunk)
            every[s, t, :, at] = combined(s, t, at).astype(jnp.bfloat16)
            return carry

        lax.fori_loop(0, width // chunk, body, 0)
        core_copy(y, t).start()

    order = []
    for dist in range(n_tp - 1, -1, -1):
        for side in (1, -1) if dist else (1,):
            t = tp + side * dist
            order.append((jnp.logical_and(t >= 0, t < n_tp), t, side, dist))

    def y_copy_b(t):
        return remote(work.at[yo, t, rows_b], yb.at[t], ysend.at[t], yrecv.at[t], (grp, y_other, tp))

    def y_copy_a():
        return remote(work.at[yo, tp, rows_a], ya, ysend.at[n_tp], yrecv.at[n_tp], (grp, y_other, tp))

    def local(y, t):
        s = y * 2 + core
        core_copy(y, t).wait_recv()

        def body(i, carry):
            at = pl.ds(pl.multiple_of(i * chunk, chunk), chunk)
            both = combined(s, t, at) + from_core[y, t, :, at].astype(jnp.float32)
            work[y, t, :, at] = both.astype(jnp.bfloat16)
            return carry

        lax.fori_loop(0, width // chunk, body, 0)

    def z_copy(part, y, t, side):
        buf, ss, rs, rows = ((za, asend, arecv, rows_a), (zb, bsend, brecv, rows_b))[part]
        if side == 1:
            slot, target = t, ups
        else:
            slot = jnp.where(t == tp - 1, n_tp, t)
            target = downs
        row = y if part == 0 else 0
        return remote(work.at[y, t, rows], buf.at[row, slot], ss.at[row, t], rs.at[row, slot], target)

    def take_z(part, y, t, slot):
        buf, ss, rs, rows = ((za, asend, arecv, rows_a), (zb, bsend, brecv, rows_b))[part]
        row = y if part == 0 else 0
        remote(work.at[y, t, rows], buf.at[row, slot], ss.at[row, t], rs.at[row, slot], ups).wait_recv()
        add_into(work.at[y, t, rows], buf.at[row, slot])

    def z_step(part, y, t, side):
        inner = tp > 0 if side == 1 else tp + 1 < n_tp
        pl.when(inner)(lambda: take_z(part, y, t, t))
        z_copy(part, y, t, side).start()

    def z_end(part, y):
        pl.when(down_ok)(lambda: take_z(part, y, tp, tp))
        pl.when(up_ok)(lambda: take_z(part, y, tp, n_tp))

    for y in (yo, yy):
        for ok, t, side, dist in order:
            pl.when(ok)(functools.partial(combine_away, y, t))
        if y is yo:
            for ok, t, side, dist in order:
                @pl.when(ok)
                def _(t=t):
                    local(yo, t)
                    y_copy_b(t).start()
    for ok, t, side, dist in order:
        @pl.when(ok)
        def _(t=t, side=side, dist=dist):
            local(yy, t)
            y_copy_b(t).wait_recv()
            add_into(work.at[yy, t, rows_b], yb.at[t])
            if dist:
                z_step(1, yy, t, side)
                z_step(0, yo, t, side)
                z_step(0, yy, t, side)
    z_end(0, yo)
    y_copy_a().start()
    z_end(0, yy)
    z_end(1, yy)
    y_copy_a().wait_recv()
    add_into(work.at[yy, tp, rows_a], ya)
    last = pltpu.make_async_copy(work.at[yy, tp], out_ref, own.at[0, 0])
    last.start()
    last.wait()
    y_copy_a().wait_send()
    for ok, t, side, dist in order:
        @pl.when(ok)
        def _(t=t, side=side, dist=dist):
            core_copy(yo, t).wait_send()
            core_copy(yy, t).wait_send()
            y_copy_b(t).wait_send()
            if dist:
                z_copy(0, yo, t, side).wait_send()
                z_copy(0, yy, t, side).wait_send()
                z_copy(1, yy, t, side).wait_send()


def add_into(dst, src):
    rows = dst.shape[0]
    strip = 16

    def body(i, carry):
        at = pl.ds(pl.multiple_of(i * strip, strip), strip)
        dst[at] = (dst[at].astype(jnp.float32) + src[at].astype(jnp.float32)).astype(dst.dtype)
        return carry

    lax.fori_loop(0, rows // strip, body, 0)


def dense_experts(normed, routes, route_weight, w_gate, w_up, w_down):
    n_sp, n_tp = lax.axis_size("sp"), lax.axis_size("tp")
    tok, width = normed.shape
    local_experts, _, hidden = w_gate.shape
    n_experts = local_experts * n_sp
    flat_route = routes.reshape(-1)
    onehot = (flat_route[:, None] == lax.iota(jnp.int32, n_experts)[None, :]).astype(jnp.int32)
    rank = jnp.sum((jnp.cumsum(onehot, axis=0) - onehot) * onehot, axis=1).reshape(tok, TOP)
    place = (routes * SLOT + rank).astype(jnp.float32)
    meta = jnp.concatenate([place, route_weight, jnp.zeros((tok, 8 - 2 * TOP), jnp.float32)], axis=1).T
    cuts = ((0, Y_FIRST), (Y_FIRST, tok - Y_FIRST))
    an, bn = cuts[0][1], cuts[1][1]
    vmem, hbm = pl.BlockSpec(memory_space=pltpu.VMEM), pl.BlockSpec(memory_space=pl.ANY)
    kind = normed.dtype
    slots, buffers = local_experts * SLOT, min(4, local_experts)
    dma = pltpu.SemaphoreType.DMA
    mixed = pl.pallas_call(
        functools.partial(layer_kernel, n_tp, cuts),
        out_shape=jax.ShapeDtypeStruct((tok, width), kind),
        in_specs=[vmem, vmem, hbm, hbm, hbm],
        out_specs=vmem,
        scratch_shapes=[
            pltpu.VMEM((4, n_tp, tok, width), kind),
            pltpu.VMEM((4, n_tp) + meta.shape, jnp.float32),
            pltpu.VMEM((4, n_tp, slots, tok), kind),
            pltpu.VMEM((local_experts, 4 * n_tp * SLOT, 128), jnp.float32),
            pltpu.VMEM((local_experts, 4 * n_tp * SLOT, width), kind),
            pltpu.VMEM((buffers, width, hidden), kind),
            pltpu.VMEM((buffers, width, hidden), kind),
            pltpu.VMEM((buffers, hidden, width), kind),
            pltpu.VMEM((2, n_tp, tok, width), kind),
            pltpu.VMEM((2, n_tp, tok, width), kind),
            pltpu.VMEM((2, n_tp + 1, an, width), kind),
            pltpu.VMEM((1, n_tp + 1, bn, width), kind),
            pltpu.VMEM((an, width), kind),
            pltpu.VMEM((n_tp, bn, width), kind),
            dma((4, n_tp, 2, 4)),
            dma((4, n_tp, 2)),
            dma((4 * n_tp - 1,)),
            dma((4 * n_tp - 1,)),
            dma((3, buffers)),
            dma((2, n_tp)),
            dma((2, n_tp)),
            dma((2, n_tp)),
            dma((2, n_tp + 1)),
            dma((1, n_tp)),
            dma((1, n_tp + 1)),
            dma((n_tp + 1,)),
            dma((n_tp + 1,)),
            dma((2, max(2, n_tp))),
        ],
        compiler_params=pltpu.CompilerParams(
            collective_id=0, has_side_effects=True, vmem_limit_bytes=56 * 2**20
        ),
        name="routed_experts",
    )(normed, meta, w_gate, w_up, w_down)
    return mixed.astype(jnp.float32)


def per_device(
    resid_in,
    pool_input,
    pool_weight,
    pool_scale,
    out_weight,
    mix_gain,
    ffn_gain,
    w_gate,
    w_up,
    w_down,
    routes,
    route_weight,
    post_gain,
):
    n_sp = lax.axis_size("sp")
    n_tp = lax.axis_size("tp")
    seg_rows, channels = pool_input.shape
    last_rows = pool_input[seg_rows - reach_back :]
    before = passed_along(last_rows, "sp", 1)
    extended = jnp.concatenate([before, pool_input], axis=0).astype(jnp.float32)
    first_chan = lax.axis_index("tp") * channels
    chan_group = (first_chan + lax.iota(jnp.int32, channels)) // GROUP_DIM
    positions = lax.axis_index("sp") * seg_rows + lax.iota(jnp.int32, seg_rows)
    window = jnp.zeros((channels,), jnp.int32)
    for group_level, win_len in enumerate(pool_windows):
        window = jnp.where(chan_group == group_level, win_len, window)
    running = jnp.zeros((seg_rows, channels), jnp.float32)
    window_sum = running
    for offset in range(pool_windows[-1]):
        running = running + extended[reach_back - offset : reach_back - offset + seg_rows]
        if offset + 1 in pool_windows:
            window_sum = jnp.where(window[None, :] == offset + 1, running, window_sum)
    divisor = jnp.minimum(positions[:, None] + 1, window[None, :]).astype(jnp.float32)
    mixed_rows = (window_sum / divisor - extended[reach_back:]).astype(jnp.bfloat16)
    token_mixed = lax.all_to_all(mixed_rows, "tp", split_axis=0, concat_axis=1, tiled=True)
    tok_rows = token_mixed.shape[0]
    pooled = jnp.einsum(
        "tgc,gcd->tgd",
        token_mixed.reshape(tok_rows, GROUPS, GROUP_DIM),
        pool_weight,
        preferred_element_type=jnp.float32,
    )
    pooled = (
        (pooled * pool_scale.reshape(GROUPS, GROUP_DIM)).astype(jnp.bfloat16).reshape(tok_rows, -1)
    )
    mix_out = jnp.dot(pooled, out_weight, preferred_element_type=jnp.float32)
    residual = (resid_in.astype(jnp.float32) + rms_scale(mix_out, mix_gain)).astype(jnp.bfloat16)
    normed = rms_scale(residual.astype(jnp.float32), ffn_gain).astype(jnp.bfloat16)
    width = normed.shape[1]
    if n_sp == 4 and n_tp <= 4 and tok_rows == 128 and w_gate.shape[2] <= 256 and w_gate.shape[0] <= 8 and tok_rows * width <= 128 * 2048:
        expert_mix = dense_experts(normed, routes, route_weight, w_gate, w_up, w_down)
        return (residual.astype(jnp.float32) + rms_scale(expert_mix, post_gain)).astype(jnp.bfloat16)
    local_experts = w_gate.shape[0]
    n_experts = local_experts * n_sp
    slot_total = n_experts * CAP
    flat_route = routes.reshape(-1)
    onehot = (flat_route[:, None] == lax.iota(jnp.int32, n_experts)[None, :]).astype(jnp.int32)
    slot_rank = jnp.sum((jnp.cumsum(onehot, axis=0) - onehot) * onehot, axis=1)
    slot_index = flat_route * CAP + slot_rank
    picker = slot_index[:, None] == lax.iota(jnp.int32, slot_total)[None, :]
    picker_rows = picker.astype(jnp.bfloat16)
    token_pick = jnp.sum(
        picker.reshape(tok_rows, TOP, slot_total).astype(jnp.float32), axis=1
    ).astype(jnp.bfloat16)
    buffer = lax.dot_general(
        token_pick, normed, (((0,), (0,)), ((), ())), preferred_element_type=jnp.float32
    )
    outgoing = buffer.astype(jnp.bfloat16).reshape(n_sp, local_experts * CAP, width)
    at_owner = lax.all_to_all(outgoing, "sp", split_axis=0, concat_axis=0, tiled=True)
    arrived = lax.all_gather(at_owner[:, None], "tp", axis=1, tiled=True)
    arrived = arrived.reshape(n_sp, n_tp, local_experts, CAP, width)
    gate_pre = jnp.einsum("sklcd,ldf->sklcf", arrived, w_gate, preferred_element_type=jnp.float32)
    upward = jnp.einsum("sklcd,ldf->sklcf", arrived, w_up, preferred_element_type=jnp.float32)
    activated = clamped_unit(gate_pre, upward).astype(jnp.bfloat16)
    terms = jnp.einsum("sklcf,lfd->kslcd", activated, w_down, preferred_element_type=jnp.float32)
    summed = lax.psum_scatter(
        terms.reshape(1 * lax.axis_size("tp"), n_sp, local_experts * CAP, width).astype(
            jnp.bfloat16
        ),
        "tp",
        scatter_dimension=0,
        tiled=True,
    ).astype(jnp.float32)
    results = summed[0].astype(jnp.bfloat16)
    returned = lax.all_to_all(results, "sp", split_axis=0, concat_axis=0, tiled=True).reshape(
        slot_total, width
    )
    gathered = jnp.dot(picker_rows, returned, preferred_element_type=jnp.float32)
    expert_mix = jnp.sum(gathered.reshape(tok_rows, TOP, width) * route_weight[:, :, None], axis=1)
    return (residual.astype(jnp.float32) + rms_scale(expert_mix, post_gain)).astype(jnp.bfloat16)


def solution(mesh):
    in_specs = (
        P(("grp", "sp", "tp"), None),
        P(("grp", "sp"), "tp"),
        P(),
        P(),
        P(),
        P(),
        P(),
        P("sp", None, "tp"),
        P("sp", None, "tp"),
        P("sp", "tp", None),
        P(("grp", "sp", "tp"), None),
        P(("grp", "sp", "tp"), None),
        P(),
    )
    out_specs = P(("grp", "sp", "tp"), None)
    return jax.shard_map(
        per_device, mesh=mesh, in_specs=in_specs, out_specs=out_specs, check_vma=False
    )
```

```python
import functools

import jax
import jax.numpy as jnp
from jax import lax
from jax.experimental import pallas as pl
from jax.experimental.pallas import tpu as pltpu
from jax.sharding import PartitionSpec as P

GROUPS = 4
GROUP_DIM = 256
TOP = 2
CAP = 9


pool_windows = (2, 4, 8, 16)
reach_back = 15
norm_eps = 1e-06
clamp_limit = 7.0
glu_alpha = 1.702


def passed_along(x, axis, by):
    size = lax.axis_size(axis)
    pairs = [(i, i + by) for i in range(size) if 0 <= i + by < size]
    return lax.ppermute(x, axis, pairs)


def rms_scale(values, gain_vec):
    inverse = lax.rsqrt(jnp.mean(values * values, axis=-1, keepdims=True) + norm_eps)
    return values * inverse * gain_vec


def clamped_unit(gate_pre, upward):
    gate_clip = jnp.minimum(gate_pre, clamp_limit)
    linear = jnp.clip(upward, -clamp_limit, clamp_limit)
    return gate_clip * jax.nn.sigmoid(glu_alpha * gate_clip) * (linear + 1.0)


SLOT = 16
Y_FIRST = 16
Z_PART = 64
MESH = pl.DeviceIdType.MESH


def coords():
    return lax.axis_index("grp"), lax.axis_index("sp"), lax.axis_index("tp")


def layer_kernel(n_tp, cuts, row_ref, meta_ref, wg_ref, wu_ref, wd_ref, out_ref,
                 every, metas, picks, weights, held, wg, wu, wd,
                 work, from_core, za, zb, ya, yb,
                 send, recv, msend, mrecv, wsem,
                 csend, crecv, asend, arecv, bsend, brecv, ysend, yrecv, own):
    grp, sp, tp = coords()
    yy, core = sp // 2, sp % 2
    yo = 1 - yy
    y_other = yo * 2 + core
    c_other = yy * 2 + (1 - core)
    tok, width = row_ref.shape
    local_experts, buffers = wg_ref.shape[0], wg.shape[0]
    slots = local_experts * SLOT
    chunk = min(512, width)
    others = [(a, b) for a in range(4) for b in range(n_tp) if (a, b) != (0, 0)]

    def weight_copies(e):
        at = lax.rem(e, buffers)
        return [pltpu.make_async_copy(w.at[e], buf.at[at], wsem.at[i, at])
                for i, (w, buf) in enumerate(((wg_ref, wg), (wu_ref, wu), (wd_ref, wd)))]

    own_copy = pltpu.make_async_copy(row_ref, every.at[sp, tp], own.at[0, 0])
    own_copy.start()
    own_meta = pltpu.make_async_copy(meta_ref, metas.at[sp, tp], own.at[0, 1])
    own_meta.start()
    barrier = pltpu.get_barrier_semaphore()
    for by in others:
        target = (grp, (sp + by[0]) % 4, (tp + by[1]) % n_tp)
        pl.semaphore_signal(barrier, inc=1, device_id=target, device_id_type=MESH)
    pl.semaphore_wait(barrier, len(others))

    def meta_copy(number, by):
        return pltpu.make_async_remote_copy(
            src_ref=meta_ref, dst_ref=metas.at[sp, tp],
            send_sem=msend.at[number], recv_sem=mrecv.at[number],
            device_id=(grp, (sp + by[0]) % 4, (tp + by[1]) % n_tp), device_id_type=MESH)

    own_copy.wait()
    own_meta.wait()

    def copy(s, t, part, way):
        target = [(grp, sp, tp + 1), (grp, sp, tp - 1), (grp, y_other, tp), (grp, c_other, tp)][way]
        first, count = cuts[part]
        piece = every.at[s, t, pl.ds(first, count)]
        return pltpu.make_async_remote_copy(
            src_ref=piece, dst_ref=piece,
            send_sem=send.at[s, t, part, way], recv_sem=recv.at[s, t, part],
            device_id=target, device_id_type=MESH)

    def arrived(s, t, part):
        copy(s, t, part, 3).wait_recv()

    sent = []

    def push(cond, s, t, part, way):
        if way == 0:
            cond = jnp.logical_and(cond, tp + 1 < n_tp)
        if way == 1:
            cond = jnp.logical_and(cond, tp > 0)
        pl.when(cond)(lambda: copy(s, t, part, way).start())
        sent.append((cond, s, t, part, way))

    def source_rows(s, t):
        return pl.ds(pl.multiple_of((s * n_tp + t) * SLOT, SLOT), SLOT)

    def select(s, t):
        slot = lax.broadcasted_iota(jnp.int32, (slots, tok), 0).astype(jnp.float32)
        base = (sp * slots).astype(jnp.float32)
        meta = metas[s, t]
        pick = jnp.zeros((slots, tok), jnp.float32)
        weight = jnp.zeros((slots, tok), jnp.float32)
        for k in range(TOP):
            hit = (meta[k : k + 1] - base) == slot
            pick = pick + jnp.where(hit, 1.0, 0.0)
            weight = weight + jnp.where(hit, meta[TOP + k : TOP + k + 1], 0.0)
        weight = jnp.broadcast_to(jnp.sum(weight, axis=1, keepdims=True), (slots, 128))
        pick = pick.astype(jnp.bfloat16)
        picks[s, t] = pick
        for e in range(local_experts):
            weights[e, source_rows(s, t)] = weight[e * SLOT : (e + 1) * SLOT]

        def body(i, carry):
            at = pl.ds(pl.multiple_of(i * chunk, chunk), chunk)
            got = jnp.dot(pick, every[s, t, :, at], preferred_element_type=jnp.float32)
            got = got.astype(jnp.bfloat16)
            for e in range(local_experts):
                held[e, source_rows(s, t), at] = got[e * SLOT : (e + 1) * SLOT]
            return carry

        lax.fori_loop(0, width // chunk, body, 0)

    yes = tp >= 0
    for number, by in enumerate(others):
        meta_copy(number, by).start()
    push(yes, sp, tp, 0, 2)
    for part in (1, 2):
        push(yes, sp, tp, part, 0)
        push(yes, sp, tp, part, 1)
        push(yes, sp, tp, part, 2)
    push(yes, sp, tp, 0, 0)
    push(yes, sp, tp, 0, 1)
    for part in (0, 1, 2):
        push(yes, sp, tp, part, 3)
    for e in range(min(buffers, local_experts)):
        for c in weight_copies(e):
            c.start()
    arrived(y_other, tp, 0)
    push(yes, y_other, tp, 0, 0)
    push(yes, y_other, tp, 0, 1)
    push(yes, y_other, tp, 0, 3)
    select(sp, tp)
    for number, by in enumerate(others):
        meta_copy(number, by).wait()

    def sides(dist):
        if dist == 0:
            return ((tp, yes),)
        return ((tp - dist, tp >= dist), (tp + dist, tp + dist < n_tp))

    def over_y(dist):
        for t, cond in sides(dist):
            for part in (1, 2):
                pl.when(cond)(functools.partial(arrived, y_other, t, part))
                push(cond, y_other, t, part, 3)
            pl.when(cond)(functools.partial(select, y_other, t))

    def cross(s, t):
        for part in (0, 1, 2):
            arrived(s, t, part)
        select(s, t)

    def over_core(s, dist):
        for t, cond in sides(dist):
            pl.when(cond)(functools.partial(cross, s, t))

    far_core = yo * 2 + (1 - core)
    for dist in range(1, n_tp):
        for s, part in ((sp, 1), (sp, 2), (sp, 0), (y_other, 0)):
            for way, (t, cond) in enumerate(sides(dist)):
                pl.when(cond)(functools.partial(arrived, s, t, part))
                push(cond, s, t, part, way)
                if part:
                    push(cond, s, t, part, 2)
                push(cond, s, t, part, 3)
        for t, cond in sides(dist):
            pl.when(cond)(functools.partial(select, sp, t))
        over_core(c_other, dist - 1)
        over_y(dist - 1)
        if dist > 1:
            over_core(far_core, dist - 2)
    over_core(c_other, n_tp - 1)
    if n_tp > 1:
        over_core(far_core, n_tp - 2)
    over_y(n_tp - 1)
    over_core(far_core, n_tp - 1)
    for cond, s, t, part, way in sent:
        pl.when(cond)(lambda s=s, t=t, part=part, way=way: copy(s, t, part, way).wait_send())

    def expert(e, carry):
        at = lax.rem(e, buffers)
        for c in weight_copies(e):
            c.wait()
        rows = held[e]
        gate_pre = jnp.dot(rows, wg[at], preferred_element_type=jnp.float32)
        upward = jnp.dot(rows, wu[at], preferred_element_type=jnp.float32)
        scale = jnp.concatenate([weights[e]] * (gate_pre.shape[1] // 128), axis=1)
        activated = (clamped_unit(gate_pre, upward) * scale).astype(jnp.bfloat16)

        def down(i, inner):
            cols = pl.ds(pl.multiple_of(i * chunk, chunk), chunk)
            term = jnp.dot(activated, wd[at, :, cols], preferred_element_type=jnp.float32)
            held[e, :, cols] = term.astype(jnp.bfloat16)
            return inner

        lax.fori_loop(0, width // chunk, down, 0)

        @pl.when(e + buffers < local_experts)
        def _():
            for c in weight_copies(e + buffers):
                c.start()

        return carry

    lax.fori_loop(0, local_experts, expert, 0)

    def combined(s, t, at):
        term = held[:, source_rows(s, t), at].reshape(slots, chunk)
        return lax.dot_general(picks[s, t], term, (((0,), (0,)), ((), ())),
                               preferred_element_type=jnp.float32)

    rows_of = [pl.ds(first, count) for first, count in cuts]
    rows_a = rows_of[0]
    ups, downs = (grp, sp, tp + 1), (grp, sp, tp - 1)
    up_ok, down_ok = tp + 1 < n_tp, tp > 0

    def remote(src, dst, s_sem, r_sem, target):
        return pltpu.make_async_remote_copy(
            src_ref=src, dst_ref=dst, send_sem=s_sem, recv_sem=r_sem,
            device_id=target, device_id_type=MESH)

    def core_copy(y, t):
        return remote(every.at[y * 2 + (1 - core), t], from_core.at[y, t],
                      csend.at[y, t], crecv.at[y, t], (grp, c_other, tp))

    def combine_away(y, t):
        s = y * 2 + (1 - core)

        def body(i, carry):
            at = pl.ds(pl.multiple_of(i * chunk, chunk), chunk)
            every[s, t, :, at] = combined(s, t, at).astype(jnp.bfloat16)
            return carry

        lax.fori_loop(0, width // chunk, body, 0)
        core_copy(y, t).start()

    order = []
    for dist in range(n_tp - 1, -1, -1):
        for side in (1, -1) if dist else (1,):
            t = tp + side * dist
            order.append((jnp.logical_and(t >= 0, t < n_tp), t, side, dist))

    def y_copy_b(part, t):
        rows = rows_of[part]
        return remote(work.at[yo, t, rows], yb.at[t, rows], ysend.at[part, t], yrecv.at[part, t],
                      (grp, y_other, tp))

    def y_copy_a():
        return remote(work.at[yo, tp, rows_a], ya, ysend.at[0, 0], yrecv.at[0, 0], (grp, y_other, tp))

    def local(y, t):
        s = y * 2 + core
        core_copy(y, t).wait_recv()

        def body(i, carry):
            at = pl.ds(pl.multiple_of(i * chunk, chunk), chunk)
            both = combined(s, t, at) + from_core[y, t, :, at].astype(jnp.float32)
            work[y, t, :, at] = both.astype(jnp.bfloat16)
            return carry

        lax.fori_loop(0, width // chunk, body, 0)

    def z_ends(part, y, t, slot):
        rows = rows_of[part]
        if part:
            return work.at[y, t, rows], zb.at[slot, rows], bsend.at[part, t], brecv.at[part, slot]
        return work.at[y, t, rows], za.at[y, slot], asend.at[y, t], arecv.at[y, slot]

    def z_copy(part, y, t, side):
        if side == 1:
            slot, target = t, ups
        else:
            slot, target = jnp.where(t == tp - 1, n_tp, t), downs
        return remote(*z_ends(part, y, t, slot), target)

    def take_z(part, y, t, slot):
        remote(*z_ends(part, y, t, slot), ups).wait_recv()
        dst, src = z_ends(part, y, t, slot)[:2]
        add_into(dst, src)

    def z_step(part, y, t, side):
        inner = tp > 0 if side == 1 else tp + 1 < n_tp
        pl.when(inner)(lambda: take_z(part, y, t, t))
        z_copy(part, y, t, side).start()

    def z_end(part, y):
        pl.when(down_ok)(lambda: take_z(part, y, tp, tp))
        pl.when(up_ok)(lambda: take_z(part, y, tp, n_tp))

    for y in (yo, yy):
        for ok, t, side, dist in order:
            pl.when(ok)(functools.partial(combine_away, y, t))
        if y is yo:
            for ok, t, side, dist in order:
                @pl.when(ok)
                def _(t=t):
                    local(yo, t)
                    y_copy_b(1, t).start()
                    y_copy_b(2, t).start()
    for ok, t, side, dist in order:
        @pl.when(ok)
        def _(t=t, side=side, dist=dist):
            local(yy, t)
            if dist:
                z_step(0, yo, t, side)
                z_step(0, yy, t, side)
            for part in (1, 2):
                y_copy_b(part, t).wait_recv()
                add_into(work.at[yy, t, rows_of[part]], yb.at[t, rows_of[part]])
                if dist:
                    z_step(part, yy, t, side)
    z_end(0, yo)
    y_copy_a().start()
    z_end(0, yy)
    z_end(1, yy)
    z_end(2, yy)
    y_copy_a().wait_recv()
    add_into(work.at[yy, tp, rows_a], ya)
    last = pltpu.make_async_copy(work.at[yy, tp], out_ref, own.at[0, 0])
    last.start()
    last.wait()
    y_copy_a().wait_send()
    for ok, t, side, dist in order:
        @pl.when(ok)
        def _(t=t, side=side, dist=dist):
            core_copy(yo, t).wait_send()
            core_copy(yy, t).wait_send()
            y_copy_b(1, t).wait_send()
            y_copy_b(2, t).wait_send()
            if dist:
                z_copy(0, yo, t, side).wait_send()
                z_copy(0, yy, t, side).wait_send()
                z_copy(1, yy, t, side).wait_send()
                z_copy(2, yy, t, side).wait_send()


def add_into(dst, src):
    rows = dst.shape[0]
    strip = 16

    def body(i, carry):
        at = pl.ds(pl.multiple_of(i * strip, strip), strip)
        dst[at] = (dst[at].astype(jnp.float32) + src[at].astype(jnp.float32)).astype(dst.dtype)
        return carry

    lax.fori_loop(0, rows // strip, body, 0)


def dense_experts(normed, routes, route_weight, w_gate, w_up, w_down):
    n_sp, n_tp = lax.axis_size("sp"), lax.axis_size("tp")
    tok, width = normed.shape
    local_experts, _, hidden = w_gate.shape
    n_experts = local_experts * n_sp
    flat_route = routes.reshape(-1)
    onehot = (flat_route[:, None] == lax.iota(jnp.int32, n_experts)[None, :]).astype(jnp.int32)
    rank = jnp.sum((jnp.cumsum(onehot, axis=0) - onehot) * onehot, axis=1).reshape(tok, TOP)
    place = (routes * SLOT + rank).astype(jnp.float32)
    meta = jnp.concatenate([place, route_weight, jnp.zeros((tok, 8 - 2 * TOP), jnp.float32)], axis=1).T
    cuts = ((0, Y_FIRST), (Y_FIRST, Z_PART), (Y_FIRST + Z_PART, tok - Y_FIRST - Z_PART))
    an = cuts[0][1]
    vmem, hbm = pl.BlockSpec(memory_space=pltpu.VMEM), pl.BlockSpec(memory_space=pl.ANY)
    kind = normed.dtype
    slots, buffers = local_experts * SLOT, min(4, local_experts)
    dma = pltpu.SemaphoreType.DMA
    mixed = pl.pallas_call(
        functools.partial(layer_kernel, n_tp, cuts),
        out_shape=jax.ShapeDtypeStruct((tok, width), kind),
        in_specs=[vmem, vmem, hbm, hbm, hbm],
        out_specs=vmem,
        scratch_shapes=[
            pltpu.VMEM((4, n_tp, tok, width), kind),
            pltpu.VMEM((4, n_tp) + meta.shape, jnp.float32),
            pltpu.VMEM((4, n_tp, slots, tok), kind),
            pltpu.VMEM((local_experts, 4 * n_tp * SLOT, 128), jnp.float32),
            pltpu.VMEM((local_experts, 4 * n_tp * SLOT, width), kind),
            pltpu.VMEM((buffers, width, hidden), kind),
            pltpu.VMEM((buffers, width, hidden), kind),
            pltpu.VMEM((buffers, hidden, width), kind),
            pltpu.VMEM((2, n_tp, tok, width), kind),
            pltpu.VMEM((2, n_tp, tok, width), kind),
            pltpu.VMEM((2, n_tp + 1, an, width), kind),
            pltpu.VMEM((n_tp + 1, tok, width), kind),
            pltpu.VMEM((an, width), kind),
            pltpu.VMEM((n_tp, tok, width), kind),
            dma((4, n_tp, 3, 4)),
            dma((4, n_tp, 3)),
            dma((4 * n_tp - 1,)),
            dma((4 * n_tp - 1,)),
            dma((3, buffers)),
            dma((2, n_tp)),
            dma((2, n_tp)),
            dma((2, n_tp)),
            dma((2, n_tp + 1)),
            dma((3, n_tp)),
            dma((3, n_tp + 1)),
            dma((3, n_tp)),
            dma((3, n_tp)),
            dma((2, max(2, n_tp))),
        ],
        compiler_params=pltpu.CompilerParams(
            collective_id=0, has_side_effects=True, vmem_limit_bytes=56 * 2**20
        ),
        name="routed_experts",
    )(normed, meta, w_gate, w_up, w_down)
    return mixed.astype(jnp.float32)


def per_device(
    resid_in,
    pool_input,
    pool_weight,
    pool_scale,
    out_weight,
    mix_gain,
    ffn_gain,
    w_gate,
    w_up,
    w_down,
    routes,
    route_weight,
    post_gain,
):
    n_sp = lax.axis_size("sp")
    n_tp = lax.axis_size("tp")
    seg_rows, channels = pool_input.shape
    last_rows = pool_input[seg_rows - reach_back :]
    before = passed_along(last_rows, "sp", 1)
    extended = jnp.concatenate([before, pool_input], axis=0).astype(jnp.float32)
    first_chan = lax.axis_index("tp") * channels
    chan_group = (first_chan + lax.iota(jnp.int32, channels)) // GROUP_DIM
    positions = lax.axis_index("sp") * seg_rows + lax.iota(jnp.int32, seg_rows)
    window = jnp.zeros((channels,), jnp.int32)
    for group_level, win_len in enumerate(pool_windows):
        window = jnp.where(chan_group == group_level, win_len, window)
    running = jnp.zeros((seg_rows, channels), jnp.float32)
    window_sum = running
    for offset in range(pool_windows[-1]):
        running = running + extended[reach_back - offset : reach_back - offset + seg_rows]
        if offset + 1 in pool_windows:
            window_sum = jnp.where(window[None, :] == offset + 1, running, window_sum)
    divisor = jnp.minimum(positions[:, None] + 1, window[None, :]).astype(jnp.float32)
    mixed_rows = (window_sum / divisor - extended[reach_back:]).astype(jnp.bfloat16)
    token_mixed = lax.all_to_all(mixed_rows, "tp", split_axis=0, concat_axis=1, tiled=True)
    tok_rows = token_mixed.shape[0]
    pooled = jnp.einsum(
        "tgc,gcd->tgd",
        token_mixed.reshape(tok_rows, GROUPS, GROUP_DIM),
        pool_weight,
        preferred_element_type=jnp.float32,
    )
    pooled = (
        (pooled * pool_scale.reshape(GROUPS, GROUP_DIM)).astype(jnp.bfloat16).reshape(tok_rows, -1)
    )
    mix_out = jnp.dot(pooled, out_weight, preferred_element_type=jnp.float32)
    residual = (resid_in.astype(jnp.float32) + rms_scale(mix_out, mix_gain)).astype(jnp.bfloat16)
    normed = rms_scale(residual.astype(jnp.float32), ffn_gain).astype(jnp.bfloat16)
    width = normed.shape[1]
    if n_sp == 4 and n_tp <= 4 and tok_rows == 128 and w_gate.shape[2] <= 256 and w_gate.shape[0] <= 8 and tok_rows * width <= 128 * 2048:
        expert_mix = dense_experts(normed, routes, route_weight, w_gate, w_up, w_down)
        return (residual.astype(jnp.float32) + rms_scale(expert_mix, post_gain)).astype(jnp.bfloat16)
    local_experts = w_gate.shape[0]
    n_experts = local_experts * n_sp
    slot_total = n_experts * CAP
    flat_route = routes.reshape(-1)
    onehot = (flat_route[:, None] == lax.iota(jnp.int32, n_experts)[None, :]).astype(jnp.int32)
    slot_rank = jnp.sum((jnp.cumsum(onehot, axis=0) - onehot) * onehot, axis=1)
    slot_index = flat_route * CAP + slot_rank
    picker = slot_index[:, None] == lax.iota(jnp.int32, slot_total)[None, :]
    picker_rows = picker.astype(jnp.bfloat16)
    token_pick = jnp.sum(
        picker.reshape(tok_rows, TOP, slot_total).astype(jnp.float32), axis=1
    ).astype(jnp.bfloat16)
    buffer = lax.dot_general(
        token_pick, normed, (((0,), (0,)), ((), ())), preferred_element_type=jnp.float32
    )
    outgoing = buffer.astype(jnp.bfloat16).reshape(n_sp, local_experts * CAP, width)
    at_owner = lax.all_to_all(outgoing, "sp", split_axis=0, concat_axis=0, tiled=True)
    arrived = lax.all_gather(at_owner[:, None], "tp", axis=1, tiled=True)
    arrived = arrived.reshape(n_sp, n_tp, local_experts, CAP, width)
    gate_pre = jnp.einsum("sklcd,ldf->sklcf", arrived, w_gate, preferred_element_type=jnp.float32)
    upward = jnp.einsum("sklcd,ldf->sklcf", arrived, w_up, preferred_element_type=jnp.float32)
    activated = clamped_unit(gate_pre, upward).astype(jnp.bfloat16)
    terms = jnp.einsum("sklcf,lfd->kslcd", activated, w_down, preferred_element_type=jnp.float32)
    summed = lax.psum_scatter(
        terms.reshape(1 * lax.axis_size("tp"), n_sp, local_experts * CAP, width).astype(
            jnp.bfloat16
        ),
        "tp",
        scatter_dimension=0,
        tiled=True,
    ).astype(jnp.float32)
    results = summed[0].astype(jnp.bfloat16)
    returned = lax.all_to_all(results, "sp", split_axis=0, concat_axis=0, tiled=True).reshape(
        slot_total, width
    )
    gathered = jnp.dot(picker_rows, returned, preferred_element_type=jnp.float32)
    expert_mix = jnp.sum(gathered.reshape(tok_rows, TOP, width) * route_weight[:, :, None], axis=1)
    return (residual.astype(jnp.float32) + rms_scale(expert_mix, post_gain)).astype(jnp.bfloat16)


def solution(mesh):
    in_specs = (
        P(("grp", "sp", "tp"), None),
        P(("grp", "sp"), "tp"),
        P(),
        P(),
        P(),
        P(),
        P(),
        P("sp", None, "tp"),
        P("sp", None, "tp"),
        P("sp", "tp", None),
        P(("grp", "sp", "tp"), None),
        P(("grp", "sp", "tp"), None),
        P(),
    )
    out_specs = P(("grp", "sp", "tp"), None)
    return jax.shard_map(
        per_device, mesh=mesh, in_specs=in_specs, out_specs=out_specs, check_vma=False
    )
```

```python
import functools

import jax
import jax.numpy as jnp
from jax import lax
from jax.experimental import pallas as pl
from jax.experimental.pallas import tpu as pltpu
from jax.sharding import PartitionSpec as P

GROUPS = 4
GROUP_DIM = 256
TOP = 2
CAP = 9


pool_windows = (2, 4, 8, 16)
reach_back = 15
norm_eps = 1e-06
clamp_limit = 7.0
glu_alpha = 1.702


def passed_along(x, axis, by):
    size = lax.axis_size(axis)
    pairs = [(i, i + by) for i in range(size) if 0 <= i + by < size]
    return lax.ppermute(x, axis, pairs)


def rms_scale(values, gain_vec):
    inverse = lax.rsqrt(jnp.mean(values * values, axis=-1, keepdims=True) + norm_eps)
    return values * inverse * gain_vec


def clamped_unit(gate_pre, upward):
    gate_clip = jnp.minimum(gate_pre, clamp_limit)
    linear = jnp.clip(upward, -clamp_limit, clamp_limit)
    return gate_clip * jax.nn.sigmoid(glu_alpha * gate_clip) * (linear + 1.0)


SLOT = 16
Y_FIRST = 16
Z_PART = 64
MESH = pl.DeviceIdType.MESH


def coords():
    return lax.axis_index("grp"), lax.axis_index("sp"), lax.axis_index("tp")


def exchange_kernel(n_tp, pool_ref, out_ref, send, recv, hsend, hrecv, own):
    grp, sp, tp = coords()
    seg_rows = pool_ref.shape[0]
    tok, reach = seg_rows // n_tp, SLOT
    first = tp == 0
    others = [(a, b) for a in range(4) for b in range(n_tp) if (a, b) != (0, 0)]
    barrier = pltpu.get_barrier_semaphore()
    for by in others:
        target = (grp, (sp + by[0]) % 4, (tp + by[1]) % n_tp)
        pl.semaphore_signal(barrier, inc=1, device_id=target, device_id_type=MESH)

    def ends(to, whole, chan):
        if whole:
            at = pl.multiple_of(to * tok - reach, reach)
            return pool_ref.at[pl.ds(at, tok + reach)], out_ref.at[chan]
        return pool_ref.at[pl.ds(0, tok)], out_ref.at[chan, pl.ds(reach, tok)]

    def main(by, whole):
        to = (tp + by) % n_tp
        src, dst = ends(to, whole, tp)
        return pltpu.make_async_remote_copy(
            src_ref=src, dst_ref=dst, send_sem=send.at[by], recv_sem=recv.at[tp],
            device_id=(grp, sp, to), device_id_type=MESH)

    def arrival(by, whole):
        chan = (tp + by) % n_tp
        src, dst = ends(1 if whole else 0, whole, chan)
        return pltpu.make_async_remote_copy(
            src_ref=src, dst_ref=dst, send_sem=send.at[by], recv_sem=recv.at[chan],
            device_id=(grp, sp, chan), device_id_type=MESH)

    def halo(chan):
        return pltpu.make_async_remote_copy(
            src_ref=pool_ref.at[pl.ds(seg_rows - reach, reach)],
            dst_ref=out_ref.at[chan, pl.ds(0, reach)],
            send_sem=hsend.at[0], recv_sem=hrecv.at[chan],
            device_id=(grp, sp + 1, 0), device_id_type=MESH)

    def kept(whole):
        src, dst = ends(tp, whole, tp)
        return pltpu.make_async_copy(src, dst, own.at[0])

    pl.semaphore_wait(barrier, len(others))
    rest = jnp.logical_not(first)
    has_next = sp + 1 < 4
    pl.when(has_next)(lambda: halo(tp).start())
    for by in range(1, n_tp):
        to_first = (tp + by) % n_tp == 0
        pl.when(to_first)(lambda by=by: main(by, False).start())
        pl.when(jnp.logical_not(to_first))(lambda by=by: main(by, True).start())
    pl.when(first)(lambda: kept(False).start())
    pl.when(rest)(lambda: kept(True).start())

    @pl.when(jnp.logical_and(first, sp == 0))
    def _():
        for chan in range(n_tp):
            out_ref[chan, pl.ds(0, reach)] = jnp.zeros((reach, out_ref.shape[2]), out_ref.dtype)

    pl.when(first)(lambda: kept(False).wait())
    pl.when(rest)(lambda: kept(True).wait())
    for by in range(1, n_tp):
        pl.when(first)(lambda by=by: arrival(by, False).wait_recv())
        pl.when(rest)(lambda by=by: arrival(by, True).wait_recv())

    @pl.when(jnp.logical_and(first, sp > 0))
    def _():
        for chan in range(n_tp):
            halo(chan).wait_recv()

    pl.when(has_next)(lambda: halo(tp).wait_send())
    for by in range(1, n_tp):
        to_first = (tp + by) % n_tp == 0
        pl.when(to_first)(lambda by=by: main(by, False).wait_send())
        pl.when(jnp.logical_not(to_first))(lambda by=by: main(by, True).wait_send())


def mixed_tokens(pool_input, pool_weight, pool_scale, n_tp):
    seg_rows, channels = pool_input.shape
    tok = seg_rows // n_tp
    vmem = pl.BlockSpec(memory_space=pltpu.VMEM)
    dma = pltpu.SemaphoreType.DMA
    rows = pl.pallas_call(
        functools.partial(exchange_kernel, n_tp),
        out_shape=jax.ShapeDtypeStruct((n_tp, tok + SLOT, channels), pool_input.dtype),
        in_specs=[vmem],
        out_specs=vmem,
        scratch_shapes=[dma((n_tp,)), dma((n_tp,)), dma((1,)), dma((n_tp,)), dma((1,))],
        compiler_params=pltpu.CompilerParams(collective_id=1, has_side_effects=True),
        name="pool_exchange",
    )(pool_input)
    start = (lax.axis_index("sp") * n_tp + lax.axis_index("tp")) * tok
    count = start + lax.broadcasted_iota(jnp.int32, (tok, 1), 0) + 1
    pooled = []
    for group, window in enumerate(pool_windows):
        held = rows[group].astype(jnp.float32)
        total = held[SLOT:]
        for offset in range(1, window):
            total = total + held[SLOT - offset : SLOT - offset + tok]
        divisor = jnp.minimum(count, window).astype(jnp.float32)
        mixed = (total / divisor - held[SLOT:]).astype(jnp.bfloat16)
        product = jnp.dot(mixed, pool_weight[group], preferred_element_type=jnp.float32)
        scale = pool_scale[group * GROUP_DIM : (group + 1) * GROUP_DIM]
        pooled.append((product * scale).astype(jnp.bfloat16))
    return jnp.concatenate(pooled, axis=1)


def routed_pool(pool_input, pool_weight, pool_scale):
    n_tp = lax.axis_size("tp")
    seg_rows, channels = pool_input.shape
    last_rows = pool_input[seg_rows - reach_back :]
    before = passed_along(last_rows, "sp", 1)
    extended = jnp.concatenate([before, pool_input], axis=0).astype(jnp.float32)
    first_chan = lax.axis_index("tp") * channels
    chan_group = (first_chan + lax.iota(jnp.int32, channels)) // GROUP_DIM
    positions = lax.axis_index("sp") * seg_rows + lax.iota(jnp.int32, seg_rows)
    window = jnp.zeros((channels,), jnp.int32)
    for group_level, win_len in enumerate(pool_windows):
        window = jnp.where(chan_group == group_level, win_len, window)
    running = jnp.zeros((seg_rows, channels), jnp.float32)
    window_sum = running
    for offset in range(pool_windows[-1]):
        running = running + extended[reach_back - offset : reach_back - offset + seg_rows]
        if offset + 1 in pool_windows:
            window_sum = jnp.where(window[None, :] == offset + 1, running, window_sum)
    divisor = jnp.minimum(positions[:, None] + 1, window[None, :]).astype(jnp.float32)
    mixed_rows = (window_sum / divisor - extended[reach_back:]).astype(jnp.bfloat16)
    token_mixed = lax.all_to_all(mixed_rows, "tp", split_axis=0, concat_axis=1, tiled=True)
    tok_rows = token_mixed.shape[0]
    pooled = jnp.einsum(
        "tgc,gcd->tgd",
        token_mixed.reshape(tok_rows, GROUPS, GROUP_DIM),
        pool_weight,
        preferred_element_type=jnp.float32,
    )
    pooled = (
        (pooled * pool_scale.reshape(GROUPS, GROUP_DIM)).astype(jnp.bfloat16).reshape(tok_rows, -1)
    )
    return pooled


def layer_kernel(n_tp, cuts, row_ref, meta_ref, wg_ref, wu_ref, wd_ref, out_ref,
                 every, metas, picks, weights, held, wg, wu, wd,
                 work, from_core, za, zb, ya, yb,
                 send, recv, msend, mrecv, wsem,
                 csend, crecv, asend, arecv, bsend, brecv, ysend, yrecv, own):
    grp, sp, tp = coords()
    yy, core = sp // 2, sp % 2
    yo = 1 - yy
    y_other = yo * 2 + core
    c_other = yy * 2 + (1 - core)
    tok, width = row_ref.shape
    local_experts, buffers = wg_ref.shape[0], wg.shape[0]
    slots = local_experts * SLOT
    chunk = min(512, width)
    others = [(a, b) for a in range(4) for b in range(n_tp) if (a, b) != (0, 0)]

    def weight_copies(e):
        at = lax.rem(e, buffers)
        return [pltpu.make_async_copy(w.at[e], buf.at[at], wsem.at[i, at])
                for i, (w, buf) in enumerate(((wg_ref, wg), (wu_ref, wu), (wd_ref, wd)))]

    own_copy = pltpu.make_async_copy(row_ref, every.at[sp, tp], own.at[0, 0])
    own_copy.start()
    own_meta = pltpu.make_async_copy(meta_ref, metas.at[sp, tp], own.at[0, 1])
    own_meta.start()
    barrier = pltpu.get_barrier_semaphore()
    for by in others:
        target = (grp, (sp + by[0]) % 4, (tp + by[1]) % n_tp)
        pl.semaphore_signal(barrier, inc=1, device_id=target, device_id_type=MESH)
    pl.semaphore_wait(barrier, len(others))

    def meta_copy(number, by):
        return pltpu.make_async_remote_copy(
            src_ref=meta_ref, dst_ref=metas.at[sp, tp],
            send_sem=msend.at[number], recv_sem=mrecv.at[number],
            device_id=(grp, (sp + by[0]) % 4, (tp + by[1]) % n_tp), device_id_type=MESH)

    own_copy.wait()
    own_meta.wait()

    def copy(s, t, part, way):
        target = [(grp, sp, tp + 1), (grp, sp, tp - 1), (grp, y_other, tp), (grp, c_other, tp)][way]
        first, count = cuts[part]
        piece = every.at[s, t, pl.ds(first, count)]
        return pltpu.make_async_remote_copy(
            src_ref=piece, dst_ref=piece,
            send_sem=send.at[s, t, part, way], recv_sem=recv.at[s, t, part],
            device_id=target, device_id_type=MESH)

    def arrived(s, t, part):
        copy(s, t, part, 3).wait_recv()

    sent = []

    def push(cond, s, t, part, way):
        if way == 0:
            cond = jnp.logical_and(cond, tp + 1 < n_tp)
        if way == 1:
            cond = jnp.logical_and(cond, tp > 0)
        pl.when(cond)(lambda: copy(s, t, part, way).start())
        sent.append((cond, s, t, part, way))

    def source_rows(s, t):
        return pl.ds(pl.multiple_of((s * n_tp + t) * SLOT, SLOT), SLOT)

    def select(s, t):
        slot = lax.broadcasted_iota(jnp.int32, (slots, tok), 0).astype(jnp.float32)
        base = (sp * slots).astype(jnp.float32)
        meta = metas[s, t]
        pick = jnp.zeros((slots, tok), jnp.float32)
        weight = jnp.zeros((slots, tok), jnp.float32)
        for k in range(TOP):
            hit = (meta[k : k + 1] - base) == slot
            pick = pick + jnp.where(hit, 1.0, 0.0)
            weight = weight + jnp.where(hit, meta[TOP + k : TOP + k + 1], 0.0)
        weight = jnp.broadcast_to(jnp.sum(weight, axis=1, keepdims=True), (slots, 128))
        pick = pick.astype(jnp.bfloat16)
        picks[s, t] = pick
        for e in range(local_experts):
            weights[e, source_rows(s, t)] = weight[e * SLOT : (e + 1) * SLOT]

        def body(i, carry):
            at = pl.ds(pl.multiple_of(i * chunk, chunk), chunk)
            got = jnp.dot(pick, every[s, t, :, at], preferred_element_type=jnp.float32)
            got = got.astype(jnp.bfloat16)
            for e in range(local_experts):
                held[e, source_rows(s, t), at] = got[e * SLOT : (e + 1) * SLOT]
            return carry

        lax.fori_loop(0, width // chunk, body, 0)

    yes = tp >= 0
    for number, by in enumerate(others):
        meta_copy(number, by).start()
    push(yes, sp, tp, 0, 2)
    for part in (1, 2):
        push(yes, sp, tp, part, 0)
        push(yes, sp, tp, part, 1)
        push(yes, sp, tp, part, 2)
    push(yes, sp, tp, 0, 0)
    push(yes, sp, tp, 0, 1)
    for part in (0, 1, 2):
        push(yes, sp, tp, part, 3)
    for e in range(min(buffers, local_experts)):
        for c in weight_copies(e):
            c.start()
    arrived(y_other, tp, 0)
    push(yes, y_other, tp, 0, 0)
    push(yes, y_other, tp, 0, 1)
    push(yes, y_other, tp, 0, 3)
    select(sp, tp)
    for number, by in enumerate(others):
        meta_copy(number, by).wait()

    def sides(dist):
        if dist == 0:
            return ((tp, yes),)
        return ((tp - dist, tp >= dist), (tp + dist, tp + dist < n_tp))

    def over_y(dist):
        for t, cond in sides(dist):
            for part in (1, 2):
                pl.when(cond)(functools.partial(arrived, y_other, t, part))
                push(cond, y_other, t, part, 3)
            pl.when(cond)(functools.partial(select, y_other, t))

    def cross(s, t):
        for part in (0, 1, 2):
            arrived(s, t, part)
        select(s, t)

    def over_core(s, dist):
        for t, cond in sides(dist):
            pl.when(cond)(functools.partial(cross, s, t))

    far_core = yo * 2 + (1 - core)
    for dist in range(1, n_tp):
        for s, part in ((sp, 1), (sp, 2), (sp, 0), (y_other, 0)):
            for way, (t, cond) in enumerate(sides(dist)):
                pl.when(cond)(functools.partial(arrived, s, t, part))
                push(cond, s, t, part, way)
                if part:
                    push(cond, s, t, part, 2)
                push(cond, s, t, part, 3)
        for t, cond in sides(dist):
            pl.when(cond)(functools.partial(select, sp, t))
        over_core(c_other, dist - 1)
        over_y(dist - 1)
        if dist > 1:
            over_core(far_core, dist - 2)
    over_core(c_other, n_tp - 1)
    if n_tp > 1:
        over_core(far_core, n_tp - 2)
    over_y(n_tp - 1)
    over_core(far_core, n_tp - 1)
    for cond, s, t, part, way in sent:
        pl.when(cond)(lambda s=s, t=t, part=part, way=way: copy(s, t, part, way).wait_send())

    def expert(e, carry):
        at = lax.rem(e, buffers)
        for c in weight_copies(e):
            c.wait()
        rows = held[e]
        gate_pre = jnp.dot(rows, wg[at], preferred_element_type=jnp.float32)
        upward = jnp.dot(rows, wu[at], preferred_element_type=jnp.float32)
        scale = jnp.concatenate([weights[e]] * (gate_pre.shape[1] // 128), axis=1)
        activated = (clamped_unit(gate_pre, upward) * scale).astype(jnp.bfloat16)

        def down(i, inner):
            cols = pl.ds(pl.multiple_of(i * chunk, chunk), chunk)
            term = jnp.dot(activated, wd[at, :, cols], preferred_element_type=jnp.float32)
            held[e, :, cols] = term.astype(jnp.bfloat16)
            return inner

        lax.fori_loop(0, width // chunk, down, 0)

        @pl.when(e + buffers < local_experts)
        def _():
            for c in weight_copies(e + buffers):
                c.start()

        return carry

    lax.fori_loop(0, local_experts, expert, 0)

    def combined(s, t, at):
        term = held[:, source_rows(s, t), at].reshape(slots, chunk)
        return lax.dot_general(picks[s, t], term, (((0,), (0,)), ((), ())),
                               preferred_element_type=jnp.float32)

    rows_of = [pl.ds(first, count) for first, count in cuts]
    rows_a = rows_of[0]
    ups, downs = (grp, sp, tp + 1), (grp, sp, tp - 1)
    up_ok, down_ok = tp + 1 < n_tp, tp > 0

    def remote(src, dst, s_sem, r_sem, target):
        return pltpu.make_async_remote_copy(
            src_ref=src, dst_ref=dst, send_sem=s_sem, recv_sem=r_sem,
            device_id=target, device_id_type=MESH)

    def core_copy(y, t):
        return remote(every.at[y * 2 + (1 - core), t], from_core.at[y, t],
                      csend.at[y, t], crecv.at[y, t], (grp, c_other, tp))

    def combine_away(y, t):
        s = y * 2 + (1 - core)

        def body(i, carry):
            at = pl.ds(pl.multiple_of(i * chunk, chunk), chunk)
            every[s, t, :, at] = combined(s, t, at).astype(jnp.bfloat16)
            return carry

        lax.fori_loop(0, width // chunk, body, 0)
        core_copy(y, t).start()

    order = []
    for dist in range(n_tp - 1, -1, -1):
        for side in (1, -1) if dist else (1,):
            t = tp + side * dist
            order.append((jnp.logical_and(t >= 0, t < n_tp), t, side, dist))

    def y_copy_b(part, t):
        rows = rows_of[part]
        return remote(work.at[yo, t, rows], yb.at[t, rows], ysend.at[part, t], yrecv.at[part, t],
                      (grp, y_other, tp))

    def y_copy_a():
        return remote(work.at[yo, tp, rows_a], ya, ysend.at[0, 0], yrecv.at[0, 0], (grp, y_other, tp))

    def local(y, t):
        s = y * 2 + core
        core_copy(y, t).wait_recv()

        def body(i, carry):
            at = pl.ds(pl.multiple_of(i * chunk, chunk), chunk)
            both = combined(s, t, at) + from_core[y, t, :, at].astype(jnp.float32)
            work[y, t, :, at] = both.astype(jnp.bfloat16)
            return carry

        lax.fori_loop(0, width // chunk, body, 0)

    def z_ends(part, y, t, slot):
        rows = rows_of[part]
        if part:
            return work.at[y, t, rows], zb.at[slot, rows], bsend.at[part, t], brecv.at[part, slot]
        return work.at[y, t, rows], za.at[y, slot], asend.at[y, t], arecv.at[y, slot]

    def z_copy(part, y, t, side):
        if side == 1:
            slot, target = t, ups
        else:
            slot, target = jnp.where(t == tp - 1, n_tp, t), downs
        return remote(*z_ends(part, y, t, slot), target)

    def take_z(part, y, t, slot):
        remote(*z_ends(part, y, t, slot), ups).wait_recv()
        dst, src = z_ends(part, y, t, slot)[:2]
        add_into(dst, src)

    def z_step(part, y, t, side):
        inner = tp > 0 if side == 1 else tp + 1 < n_tp
        pl.when(inner)(lambda: take_z(part, y, t, t))
        z_copy(part, y, t, side).start()

    def z_end(part, y):
        pl.when(down_ok)(lambda: take_z(part, y, tp, tp))
        pl.when(up_ok)(lambda: take_z(part, y, tp, n_tp))

    for y in (yo, yy):
        for ok, t, side, dist in order:
            pl.when(ok)(functools.partial(combine_away, y, t))
        if y is yo:
            for ok, t, side, dist in order:
                @pl.when(ok)
                def _(t=t):
                    local(yo, t)
                    y_copy_b(1, t).start()
                    y_copy_b(2, t).start()
    for ok, t, side, dist in order:
        @pl.when(ok)
        def _(t=t, side=side, dist=dist):
            local(yy, t)
            if dist:
                z_step(0, yo, t, side)
                z_step(0, yy, t, side)
            for part in (1, 2):
                y_copy_b(part, t).wait_recv()
                add_into(work.at[yy, t, rows_of[part]], yb.at[t, rows_of[part]])
                if dist:
                    z_step(part, yy, t, side)
    z_end(0, yo)
    y_copy_a().start()
    z_end(0, yy)
    z_end(1, yy)
    z_end(2, yy)
    y_copy_a().wait_recv()
    add_into(work.at[yy, tp, rows_a], ya)
    last = pltpu.make_async_copy(work.at[yy, tp], out_ref, own.at[0, 0])
    last.start()
    last.wait()
    y_copy_a().wait_send()
    for ok, t, side, dist in order:
        @pl.when(ok)
        def _(t=t, side=side, dist=dist):
            core_copy(yo, t).wait_send()
            core_copy(yy, t).wait_send()
            y_copy_b(1, t).wait_send()
            y_copy_b(2, t).wait_send()
            if dist:
                z_copy(0, yo, t, side).wait_send()
                z_copy(0, yy, t, side).wait_send()
                z_copy(1, yy, t, side).wait_send()
                z_copy(2, yy, t, side).wait_send()


def add_into(dst, src):
    rows = dst.shape[0]
    strip = 16

    def body(i, carry):
        at = pl.ds(pl.multiple_of(i * strip, strip), strip)
        dst[at] = (dst[at].astype(jnp.float32) + src[at].astype(jnp.float32)).astype(dst.dtype)
        return carry

    lax.fori_loop(0, rows // strip, body, 0)


def dense_experts(normed, routes, route_weight, w_gate, w_up, w_down):
    n_sp, n_tp = lax.axis_size("sp"), lax.axis_size("tp")
    tok, width = normed.shape
    local_experts, _, hidden = w_gate.shape
    n_experts = local_experts * n_sp
    flat_route = routes.reshape(-1)
    onehot = (flat_route[:, None] == lax.iota(jnp.int32, n_experts)[None, :]).astype(jnp.int32)
    rank = jnp.sum((jnp.cumsum(onehot, axis=0) - onehot) * onehot, axis=1).reshape(tok, TOP)
    place = (routes * SLOT + rank).astype(jnp.float32)
    meta = jnp.concatenate([place, route_weight, jnp.zeros((tok, 8 - 2 * TOP), jnp.float32)], axis=1).T
    cuts = ((0, Y_FIRST), (Y_FIRST, Z_PART), (Y_FIRST + Z_PART, tok - Y_FIRST - Z_PART))
    an = cuts[0][1]
    vmem, hbm = pl.BlockSpec(memory_space=pltpu.VMEM), pl.BlockSpec(memory_space=pl.ANY)
    kind = normed.dtype
    slots, buffers = local_experts * SLOT, min(4, local_experts)
    dma = pltpu.SemaphoreType.DMA
    mixed = pl.pallas_call(
        functools.partial(layer_kernel, n_tp, cuts),
        out_shape=jax.ShapeDtypeStruct((tok, width), kind),
        in_specs=[vmem, vmem, hbm, hbm, hbm],
        out_specs=vmem,
        scratch_shapes=[
            pltpu.VMEM((4, n_tp, tok, width), kind),
            pltpu.VMEM((4, n_tp) + meta.shape, jnp.float32),
            pltpu.VMEM((4, n_tp, slots, tok), kind),
            pltpu.VMEM((local_experts, 4 * n_tp * SLOT, 128), jnp.float32),
            pltpu.VMEM((local_experts, 4 * n_tp * SLOT, width), kind),
            pltpu.VMEM((buffers, width, hidden), kind),
            pltpu.VMEM((buffers, width, hidden), kind),
            pltpu.VMEM((buffers, hidden, width), kind),
            pltpu.VMEM((2, n_tp, tok, width), kind),
            pltpu.VMEM((2, n_tp, tok, width), kind),
            pltpu.VMEM((2, n_tp + 1, an, width), kind),
            pltpu.VMEM((n_tp + 1, tok, width), kind),
            pltpu.VMEM((an, width), kind),
            pltpu.VMEM((n_tp, tok, width), kind),
            dma((4, n_tp, 3, 4)),
            dma((4, n_tp, 3)),
            dma((4 * n_tp - 1,)),
            dma((4 * n_tp - 1,)),
            dma((3, buffers)),
            dma((2, n_tp)),
            dma((2, n_tp)),
            dma((2, n_tp)),
            dma((2, n_tp + 1)),
            dma((3, n_tp)),
            dma((3, n_tp + 1)),
            dma((3, n_tp)),
            dma((3, n_tp)),
            dma((2, max(2, n_tp))),
        ],
        compiler_params=pltpu.CompilerParams(
            collective_id=0, has_side_effects=True, vmem_limit_bytes=56 * 2**20
        ),
        name="routed_experts",
    )(normed, meta, w_gate, w_up, w_down)
    return mixed.astype(jnp.float32)


def per_device(
    resid_in,
    pool_input,
    pool_weight,
    pool_scale,
    out_weight,
    mix_gain,
    ffn_gain,
    w_gate,
    w_up,
    w_down,
    routes,
    route_weight,
    post_gain,
):
    n_sp = lax.axis_size("sp")
    n_tp = lax.axis_size("tp")
    seg_rows, channels = pool_input.shape
    if n_sp == 4 and n_tp == GROUPS and channels == GROUP_DIM and seg_rows == n_tp * 128:
        pooled = mixed_tokens(pool_input, pool_weight, pool_scale, n_tp)
    else:
        pooled = routed_pool(pool_input, pool_weight, pool_scale)
    tok_rows = pooled.shape[0]
    mix_out = jnp.dot(pooled, out_weight, preferred_element_type=jnp.float32)
    residual = (resid_in.astype(jnp.float32) + rms_scale(mix_out, mix_gain)).astype(jnp.bfloat16)
    normed = rms_scale(residual.astype(jnp.float32), ffn_gain).astype(jnp.bfloat16)
    width = normed.shape[1]
    if n_sp == 4 and n_tp <= 4 and tok_rows == 128 and w_gate.shape[2] <= 256 and w_gate.shape[0] <= 8 and tok_rows * width <= 128 * 2048:
        expert_mix = dense_experts(normed, routes, route_weight, w_gate, w_up, w_down)
        return (residual.astype(jnp.float32) + rms_scale(expert_mix, post_gain)).astype(jnp.bfloat16)
    local_experts = w_gate.shape[0]
    n_experts = local_experts * n_sp
    slot_total = n_experts * CAP
    flat_route = routes.reshape(-1)
    onehot = (flat_route[:, None] == lax.iota(jnp.int32, n_experts)[None, :]).astype(jnp.int32)
    slot_rank = jnp.sum((jnp.cumsum(onehot, axis=0) - onehot) * onehot, axis=1)
    slot_index = flat_route * CAP + slot_rank
    picker = slot_index[:, None] == lax.iota(jnp.int32, slot_total)[None, :]
    picker_rows = picker.astype(jnp.bfloat16)
    token_pick = jnp.sum(
        picker.reshape(tok_rows, TOP, slot_total).astype(jnp.float32), axis=1
    ).astype(jnp.bfloat16)
    buffer = lax.dot_general(
        token_pick, normed, (((0,), (0,)), ((), ())), preferred_element_type=jnp.float32
    )
    outgoing = buffer.astype(jnp.bfloat16).reshape(n_sp, local_experts * CAP, width)
    at_owner = lax.all_to_all(outgoing, "sp", split_axis=0, concat_axis=0, tiled=True)
    arrived = lax.all_gather(at_owner[:, None], "tp", axis=1, tiled=True)
    arrived = arrived.reshape(n_sp, n_tp, local_experts, CAP, width)
    gate_pre = jnp.einsum("sklcd,ldf->sklcf", arrived, w_gate, preferred_element_type=jnp.float32)
    upward = jnp.einsum("sklcd,ldf->sklcf", arrived, w_up, preferred_element_type=jnp.float32)
    activated = clamped_unit(gate_pre, upward).astype(jnp.bfloat16)
    terms = jnp.einsum("sklcf,lfd->kslcd", activated, w_down, preferred_element_type=jnp.float32)
    summed = lax.psum_scatter(
        terms.reshape(1 * lax.axis_size("tp"), n_sp, local_experts * CAP, width).astype(
            jnp.bfloat16
        ),
        "tp",
        scatter_dimension=0,
        tiled=True,
    ).astype(jnp.float32)
    results = summed[0].astype(jnp.bfloat16)
    returned = lax.all_to_all(results, "sp", split_axis=0, concat_axis=0, tiled=True).reshape(
        slot_total, width
    )
    gathered = jnp.dot(picker_rows, returned, preferred_element_type=jnp.float32)
    expert_mix = jnp.sum(gathered.reshape(tok_rows, TOP, width) * route_weight[:, :, None], axis=1)
    return (residual.astype(jnp.float32) + rms_scale(expert_mix, post_gain)).astype(jnp.bfloat16)


def solution(mesh):
    in_specs = (
        P(("grp", "sp", "tp"), None),
        P(("grp", "sp"), "tp"),
        P(),
        P(),
        P(),
        P(),
        P(),
        P("sp", None, "tp"),
        P("sp", None, "tp"),
        P("sp", "tp", None),
        P(("grp", "sp", "tp"), None),
        P(("grp", "sp", "tp"), None),
        P(),
    )
    out_specs = P(("grp", "sp", "tp"), None)
    return jax.shard_map(
        per_device, mesh=mesh, in_specs=in_specs, out_specs=out_specs, check_vma=False
    )
```

```python
import functools

import jax
import jax.numpy as jnp
from jax import lax
from jax.experimental import pallas as pl
from jax.experimental.pallas import tpu as pltpu
from jax.sharding import PartitionSpec as P

GROUPS = 4
GROUP_DIM = 256
TOP = 2
CAP = 9


pool_windows = (2, 4, 8, 16)
reach_back = 15
norm_eps = 1e-06
clamp_limit = 7.0
glu_alpha = 1.702


def passed_along(x, axis, by):
    size = lax.axis_size(axis)
    pairs = [(i, i + by) for i in range(size) if 0 <= i + by < size]
    return lax.ppermute(x, axis, pairs)


def rms_scale(values, gain_vec):
    inverse = lax.rsqrt(jnp.mean(values * values, axis=-1, keepdims=True) + norm_eps)
    return values * inverse * gain_vec


def clamped_unit(gate_pre, upward):
    gate_clip = jnp.minimum(gate_pre, clamp_limit)
    linear = jnp.clip(upward, -clamp_limit, clamp_limit)
    return gate_clip * jax.nn.sigmoid(glu_alpha * gate_clip) * (linear + 1.0)


SLOT = 16
Y_FIRST = 16
Z_PART = 64
MESH = pl.DeviceIdType.MESH


def coords():
    return lax.axis_index("grp"), lax.axis_index("sp"), lax.axis_index("tp")


def exchange_kernel(n_tp, pool_ref, out_ref, send, recv, hsend, hrecv, own):
    grp, sp, tp = coords()
    seg_rows = pool_ref.shape[0]
    tok, reach = seg_rows // n_tp, SLOT
    first = tp == 0
    others = [(a, b) for a in range(4) for b in range(n_tp) if (a, b) != (0, 0)]
    barrier = pltpu.get_barrier_semaphore()
    for by in others:
        target = (grp, (sp + by[0]) % 4, (tp + by[1]) % n_tp)
        pl.semaphore_signal(barrier, inc=1, device_id=target, device_id_type=MESH)

    def ends(to, whole, chan):
        if whole:
            at = pl.multiple_of(to * tok - reach, reach)
            return pool_ref.at[pl.ds(at, tok + reach)], out_ref.at[chan]
        return pool_ref.at[pl.ds(0, tok)], out_ref.at[chan, pl.ds(reach, tok)]

    def main(by, whole):
        to = (tp + by) % n_tp
        src, dst = ends(to, whole, tp)
        return pltpu.make_async_remote_copy(
            src_ref=src, dst_ref=dst, send_sem=send.at[by], recv_sem=recv.at[tp],
            device_id=(grp, sp, to), device_id_type=MESH)

    def arrival(by, whole):
        chan = (tp + by) % n_tp
        src, dst = ends(1 if whole else 0, whole, chan)
        return pltpu.make_async_remote_copy(
            src_ref=src, dst_ref=dst, send_sem=send.at[by], recv_sem=recv.at[chan],
            device_id=(grp, sp, chan), device_id_type=MESH)

    def halo(chan):
        return pltpu.make_async_remote_copy(
            src_ref=pool_ref.at[pl.ds(seg_rows - reach, reach)],
            dst_ref=out_ref.at[chan, pl.ds(0, reach)],
            send_sem=hsend.at[0], recv_sem=hrecv.at[chan],
            device_id=(grp, sp + 1, 0), device_id_type=MESH)

    def kept(whole):
        src, dst = ends(tp, whole, tp)
        return pltpu.make_async_copy(src, dst, own.at[0])

    pl.semaphore_wait(barrier, len(others))
    rest = jnp.logical_not(first)
    has_next = sp + 1 < 4
    pl.when(has_next)(lambda: halo(tp).start())
    for by in range(1, n_tp):
        to_first = (tp + by) % n_tp == 0
        pl.when(to_first)(lambda by=by: main(by, False).start())
        pl.when(jnp.logical_not(to_first))(lambda by=by: main(by, True).start())
    pl.when(first)(lambda: kept(False).start())
    pl.when(rest)(lambda: kept(True).start())

    @pl.when(jnp.logical_and(first, sp == 0))
    def _():
        for chan in range(n_tp):
            out_ref[chan, pl.ds(0, reach)] = jnp.zeros((reach, out_ref.shape[2]), out_ref.dtype)

    pl.when(first)(lambda: kept(False).wait())
    pl.when(rest)(lambda: kept(True).wait())
    for by in range(1, n_tp):
        pl.when(first)(lambda by=by: arrival(by, False).wait_recv())
        pl.when(rest)(lambda by=by: arrival(by, True).wait_recv())

    @pl.when(jnp.logical_and(first, sp > 0))
    def _():
        for chan in range(n_tp):
            halo(chan).wait_recv()

    pl.when(has_next)(lambda: halo(tp).wait_send())
    for by in range(1, n_tp):
        to_first = (tp + by) % n_tp == 0
        pl.when(to_first)(lambda by=by: main(by, False).wait_send())
        pl.when(jnp.logical_not(to_first))(lambda by=by: main(by, True).wait_send())


def mixed_tokens(pool_input, pool_weight, pool_scale, n_tp):
    seg_rows, channels = pool_input.shape
    tok = seg_rows // n_tp
    vmem = pl.BlockSpec(memory_space=pltpu.VMEM)
    dma = pltpu.SemaphoreType.DMA
    rows = pl.pallas_call(
        functools.partial(exchange_kernel, n_tp),
        out_shape=jax.ShapeDtypeStruct((n_tp, tok + SLOT, channels), pool_input.dtype),
        in_specs=[vmem],
        out_specs=vmem,
        scratch_shapes=[dma((n_tp,)), dma((n_tp,)), dma((1,)), dma((n_tp,)), dma((1,))],
        compiler_params=pltpu.CompilerParams(collective_id=1, has_side_effects=True),
        name="pool_exchange",
    )(pool_input)
    start = (lax.axis_index("sp") * n_tp + lax.axis_index("tp")) * tok
    count = start + lax.broadcasted_iota(jnp.int32, (tok, 1), 0) + 1
    pooled = []
    for group, window in enumerate(pool_windows):
        held = rows[group].astype(jnp.float32)
        total = held[SLOT:]
        for offset in range(1, window):
            total = total + held[SLOT - offset : SLOT - offset + tok]
        divisor = jnp.minimum(count, window).astype(jnp.float32)
        mixed = (total / divisor - held[SLOT:]).astype(jnp.bfloat16)
        product = jnp.dot(mixed, pool_weight[group], preferred_element_type=jnp.float32)
        scale = pool_scale[group * GROUP_DIM : (group + 1) * GROUP_DIM]
        pooled.append((product * scale).astype(jnp.bfloat16))
    return jnp.concatenate(pooled, axis=1)


def routed_pool(pool_input, pool_weight, pool_scale):
    n_tp = lax.axis_size("tp")
    seg_rows, channels = pool_input.shape
    last_rows = pool_input[seg_rows - reach_back :]
    before = passed_along(last_rows, "sp", 1)
    extended = jnp.concatenate([before, pool_input], axis=0).astype(jnp.float32)
    first_chan = lax.axis_index("tp") * channels
    chan_group = (first_chan + lax.iota(jnp.int32, channels)) // GROUP_DIM
    positions = lax.axis_index("sp") * seg_rows + lax.iota(jnp.int32, seg_rows)
    window = jnp.zeros((channels,), jnp.int32)
    for group_level, win_len in enumerate(pool_windows):
        window = jnp.where(chan_group == group_level, win_len, window)
    running = jnp.zeros((seg_rows, channels), jnp.float32)
    window_sum = running
    for offset in range(pool_windows[-1]):
        running = running + extended[reach_back - offset : reach_back - offset + seg_rows]
        if offset + 1 in pool_windows:
            window_sum = jnp.where(window[None, :] == offset + 1, running, window_sum)
    divisor = jnp.minimum(positions[:, None] + 1, window[None, :]).astype(jnp.float32)
    mixed_rows = (window_sum / divisor - extended[reach_back:]).astype(jnp.bfloat16)
    token_mixed = lax.all_to_all(mixed_rows, "tp", split_axis=0, concat_axis=1, tiled=True)
    tok_rows = token_mixed.shape[0]
    pooled = jnp.einsum(
        "tgc,gcd->tgd",
        token_mixed.reshape(tok_rows, GROUPS, GROUP_DIM),
        pool_weight,
        preferred_element_type=jnp.float32,
    )
    pooled = (
        (pooled * pool_scale.reshape(GROUPS, GROUP_DIM)).astype(jnp.bfloat16).reshape(tok_rows, -1)
    )
    return pooled


def layer_kernel(n_tp, cuts, row_ref, meta_ref, wg_ref, wu_ref, wd_ref, out_ref,
                 every, metas, picks, weights, held, wg, wu, wd,
                 work, from_core, za, zb, ya, yb,
                 send, recv, msend, mrecv, wsem,
                 csend, crecv, asend, arecv, bsend, brecv, ysend, yrecv, own):
    grp, sp, tp = coords()
    yy, core = sp // 2, sp % 2
    yo = 1 - yy
    y_other = yo * 2 + core
    c_other = yy * 2 + (1 - core)
    tok, width = row_ref.shape
    local_experts, buffers = wg_ref.shape[0], wg.shape[0]
    slots = local_experts * SLOT
    chunk = min(1024, width)
    others = [(a, b) for a in range(4) for b in range(n_tp) if (a, b) != (0, 0)]

    def weight_copies(e):
        at = lax.rem(e, buffers)
        return [pltpu.make_async_copy(w.at[e], buf.at[at], wsem.at[i, at])
                for i, (w, buf) in enumerate(((wg_ref, wg), (wu_ref, wu), (wd_ref, wd)))]

    own_copy = pltpu.make_async_copy(row_ref, every.at[sp, tp], own.at[0, 0])
    own_copy.start()
    own_meta = pltpu.make_async_copy(meta_ref, metas.at[sp, tp], own.at[0, 1])
    own_meta.start()
    barrier = pltpu.get_barrier_semaphore()
    for by in others:
        target = (grp, (sp + by[0]) % 4, (tp + by[1]) % n_tp)
        pl.semaphore_signal(barrier, inc=1, device_id=target, device_id_type=MESH)
    pl.semaphore_wait(barrier, len(others))

    def meta_copy(number, by):
        return pltpu.make_async_remote_copy(
            src_ref=meta_ref, dst_ref=metas.at[sp, tp],
            send_sem=msend.at[number], recv_sem=mrecv.at[number],
            device_id=(grp, (sp + by[0]) % 4, (tp + by[1]) % n_tp), device_id_type=MESH)

    own_copy.wait()
    own_meta.wait()

    def copy(s, t, part, way):
        target = [(grp, sp, tp + 1), (grp, sp, tp - 1), (grp, y_other, tp), (grp, c_other, tp)][way]
        first, count = cuts[part]
        piece = every.at[s, t, pl.ds(first, count)]
        return pltpu.make_async_remote_copy(
            src_ref=piece, dst_ref=piece,
            send_sem=send.at[s, t, part, way], recv_sem=recv.at[s, t, part],
            device_id=target, device_id_type=MESH)

    def arrived(s, t, part):
        copy(s, t, part, 3).wait_recv()

    sent = []

    def push(cond, s, t, part, way):
        if way == 0:
            cond = jnp.logical_and(cond, tp + 1 < n_tp)
        if way == 1:
            cond = jnp.logical_and(cond, tp > 0)
        pl.when(cond)(lambda: copy(s, t, part, way).start())
        sent.append((cond, s, t, part, way))

    def source_rows(s, t):
        return pl.ds(pl.multiple_of((s * n_tp + t) * SLOT, SLOT), SLOT)

    def select(s, t):
        slot = lax.broadcasted_iota(jnp.int32, (slots, tok), 0).astype(jnp.float32)
        base = (sp * slots).astype(jnp.float32)
        meta = metas[s, t]
        pick = jnp.zeros((slots, tok), jnp.float32)
        weight = jnp.zeros((slots, tok), jnp.float32)
        for k in range(TOP):
            hit = (meta[k : k + 1] - base) == slot
            pick = pick + jnp.where(hit, 1.0, 0.0)
            weight = weight + jnp.where(hit, meta[TOP + k : TOP + k + 1], 0.0)
        weight = jnp.broadcast_to(jnp.sum(weight, axis=1, keepdims=True), (slots, 128))
        pick = pick.astype(jnp.bfloat16)
        picks[s, t] = pick
        for e in range(local_experts):
            weights[e, source_rows(s, t)] = weight[e * SLOT : (e + 1) * SLOT]

        def body(i, carry):
            at = pl.ds(pl.multiple_of(i * chunk, chunk), chunk)
            got = jnp.dot(pick, every[s, t, :, at], preferred_element_type=jnp.float32)
            got = got.astype(jnp.bfloat16)
            for e in range(local_experts):
                held[e, source_rows(s, t), at] = got[e * SLOT : (e + 1) * SLOT]
            return carry

        lax.fori_loop(0, width // chunk, body, 0)

    yes = tp >= 0
    for number, by in enumerate(others):
        meta_copy(number, by).start()
    push(yes, sp, tp, 0, 2)
    for part in (1, 2):
        push(yes, sp, tp, part, 0)
        push(yes, sp, tp, part, 1)
        push(yes, sp, tp, part, 2)
    push(yes, sp, tp, 0, 0)
    push(yes, sp, tp, 0, 1)
    for part in (0, 1, 2):
        push(yes, sp, tp, part, 3)
    for e in range(min(buffers, local_experts)):
        for c in weight_copies(e):
            c.start()
    arrived(y_other, tp, 0)
    push(yes, y_other, tp, 0, 0)
    push(yes, y_other, tp, 0, 1)
    push(yes, y_other, tp, 0, 3)
    select(sp, tp)
    for number, by in enumerate(others):
        meta_copy(number, by).wait()

    def sides(dist):
        if dist == 0:
            return ((tp, yes),)
        return ((tp - dist, tp >= dist), (tp + dist, tp + dist < n_tp))

    def over_y(dist):
        for t, cond in sides(dist):
            for part in (1, 2):
                pl.when(cond)(functools.partial(arrived, y_other, t, part))
                push(cond, y_other, t, part, 3)
            pl.when(cond)(functools.partial(select, y_other, t))

    def cross(s, t):
        for part in (0, 1, 2):
            arrived(s, t, part)
        select(s, t)

    def over_core(s, dist):
        for t, cond in sides(dist):
            pl.when(cond)(functools.partial(cross, s, t))

    far_core = yo * 2 + (1 - core)
    for dist in range(1, n_tp):
        for s, part in ((sp, 1), (sp, 2), (sp, 0), (y_other, 0)):
            for way, (t, cond) in enumerate(sides(dist)):
                pl.when(cond)(functools.partial(arrived, s, t, part))
                push(cond, s, t, part, way)
                if part:
                    push(cond, s, t, part, 2)
                push(cond, s, t, part, 3)
        for t, cond in sides(dist):
            pl.when(cond)(functools.partial(select, sp, t))
        over_core(c_other, dist - 1)
        over_y(dist - 1)
        if dist > 1:
            over_core(far_core, dist - 2)
    over_core(c_other, n_tp - 1)
    if n_tp > 1:
        over_core(far_core, n_tp - 2)
    over_y(n_tp - 1)
    over_core(far_core, n_tp - 1)
    for cond, s, t, part, way in sent:
        pl.when(cond)(lambda s=s, t=t, part=part, way=way: copy(s, t, part, way).wait_send())

    def expert(e, carry):
        at = lax.rem(e, buffers)
        for c in weight_copies(e):
            c.wait()
        rows = held[e]
        gate_pre = jnp.dot(rows, wg[at], preferred_element_type=jnp.float32)
        upward = jnp.dot(rows, wu[at], preferred_element_type=jnp.float32)
        scale = jnp.concatenate([weights[e]] * (gate_pre.shape[1] // 128), axis=1)
        activated = (clamped_unit(gate_pre, upward) * scale).astype(jnp.bfloat16)

        def down(i, inner):
            cols = pl.ds(pl.multiple_of(i * chunk, chunk), chunk)
            term = jnp.dot(activated, wd[at, :, cols], preferred_element_type=jnp.float32)
            held[e, :, cols] = term.astype(jnp.bfloat16)
            return inner

        lax.fori_loop(0, width // chunk, down, 0)

        @pl.when(e + buffers < local_experts)
        def _():
            for c in weight_copies(e + buffers):
                c.start()

        return carry

    lax.fori_loop(0, local_experts, expert, 0)

    def combined(s, t, at):
        term = held[:, source_rows(s, t), at].reshape(slots, chunk)
        return lax.dot_general(picks[s, t], term, (((0,), (0,)), ((), ())),
                               preferred_element_type=jnp.float32)

    rows_of = [pl.ds(first, count) for first, count in cuts]
    rows_a = rows_of[0]
    ups, downs = (grp, sp, tp + 1), (grp, sp, tp - 1)
    up_ok, down_ok = tp + 1 < n_tp, tp > 0

    def remote(src, dst, s_sem, r_sem, target):
        return pltpu.make_async_remote_copy(
            src_ref=src, dst_ref=dst, send_sem=s_sem, recv_sem=r_sem,
            device_id=target, device_id_type=MESH)

    def core_copy(y, t):
        return remote(every.at[y * 2 + (1 - core), t], from_core.at[y, t],
                      csend.at[y, t], crecv.at[y, t], (grp, c_other, tp))

    def combine_away(y, t):
        s = y * 2 + (1 - core)

        def body(i, carry):
            at = pl.ds(pl.multiple_of(i * chunk, chunk), chunk)
            every[s, t, :, at] = combined(s, t, at).astype(jnp.bfloat16)
            return carry

        lax.fori_loop(0, width // chunk, body, 0)
        core_copy(y, t).start()

    order = []
    for dist in range(n_tp - 1, -1, -1):
        for side in (1, -1) if dist else (1,):
            t = tp + side * dist
            order.append((jnp.logical_and(t >= 0, t < n_tp), t, side, dist))

    def y_copy_b(part, t):
        rows = rows_of[part]
        return remote(work.at[yo, t, rows], yb.at[t, rows], ysend.at[part, t], yrecv.at[part, t],
                      (grp, y_other, tp))

    def y_copy_a():
        return remote(work.at[yo, tp, rows_a], ya, ysend.at[0, 0], yrecv.at[0, 0], (grp, y_other, tp))

    def local(y, t):
        s = y * 2 + core
        core_copy(y, t).wait_recv()

        def body(i, carry):
            at = pl.ds(pl.multiple_of(i * chunk, chunk), chunk)
            both = combined(s, t, at) + from_core[y, t, :, at].astype(jnp.float32)
            work[y, t, :, at] = both.astype(jnp.bfloat16)
            return carry

        lax.fori_loop(0, width // chunk, body, 0)

    def z_ends(part, y, t, slot):
        rows = rows_of[part]
        if part:
            return work.at[y, t, rows], zb.at[slot, rows], bsend.at[part, t], brecv.at[part, slot]
        return work.at[y, t, rows], za.at[y, slot], asend.at[y, t], arecv.at[y, slot]

    def z_copy(part, y, t, side):
        if side == 1:
            slot, target = t, ups
        else:
            slot, target = jnp.where(t == tp - 1, n_tp, t), downs
        return remote(*z_ends(part, y, t, slot), target)

    def take_z(part, y, t, slot):
        remote(*z_ends(part, y, t, slot), ups).wait_recv()
        dst, src = z_ends(part, y, t, slot)[:2]
        add_into(dst, src)

    def z_step(part, y, t, side):
        inner = tp > 0 if side == 1 else tp + 1 < n_tp
        pl.when(inner)(lambda: take_z(part, y, t, t))
        z_copy(part, y, t, side).start()

    def z_end(part, y):
        pl.when(down_ok)(lambda: take_z(part, y, tp, tp))
        pl.when(up_ok)(lambda: take_z(part, y, tp, n_tp))

    for y in (yo, yy):
        for ok, t, side, dist in order:
            pl.when(ok)(functools.partial(combine_away, y, t))
        if y is yo:
            for ok, t, side, dist in order:
                @pl.when(ok)
                def _(t=t):
                    local(yo, t)
                    y_copy_b(1, t).start()
                    y_copy_b(2, t).start()
    for ok, t, side, dist in order:
        @pl.when(ok)
        def _(t=t, side=side, dist=dist):
            local(yy, t)
            if dist:
                z_step(0, yo, t, side)
                z_step(0, yy, t, side)
            for part in (1, 2):
                y_copy_b(part, t).wait_recv()
                add_into(work.at[yy, t, rows_of[part]], yb.at[t, rows_of[part]])
                if dist:
                    z_step(part, yy, t, side)
    z_end(0, yo)
    y_copy_a().start()
    z_end(0, yy)
    z_end(1, yy)
    z_end(2, yy)
    y_copy_a().wait_recv()
    add_into(work.at[yy, tp, rows_a], ya)
    last = pltpu.make_async_copy(work.at[yy, tp], out_ref, own.at[0, 0])
    last.start()
    last.wait()
    y_copy_a().wait_send()
    for ok, t, side, dist in order:
        @pl.when(ok)
        def _(t=t, side=side, dist=dist):
            core_copy(yo, t).wait_send()
            core_copy(yy, t).wait_send()
            y_copy_b(1, t).wait_send()
            y_copy_b(2, t).wait_send()
            if dist:
                z_copy(0, yo, t, side).wait_send()
                z_copy(0, yy, t, side).wait_send()
                z_copy(1, yy, t, side).wait_send()
                z_copy(2, yy, t, side).wait_send()


def add_into(dst, src):
    rows = dst.shape[0]
    strip = 16

    def body(i, carry):
        at = pl.ds(pl.multiple_of(i * strip, strip), strip)
        dst[at] = (dst[at].astype(jnp.float32) + src[at].astype(jnp.float32)).astype(dst.dtype)
        return carry

    lax.fori_loop(0, rows // strip, body, 0)


def dense_experts(normed, routes, route_weight, w_gate, w_up, w_down):
    n_sp, n_tp = lax.axis_size("sp"), lax.axis_size("tp")
    tok, width = normed.shape
    local_experts, _, hidden = w_gate.shape
    n_experts = local_experts * n_sp
    flat_route = routes.reshape(-1)
    onehot = (flat_route[:, None] == lax.iota(jnp.int32, n_experts)[None, :]).astype(jnp.int32)
    rank = jnp.sum((jnp.cumsum(onehot, axis=0) - onehot) * onehot, axis=1).reshape(tok, TOP)
    place = (routes * SLOT + rank).astype(jnp.float32)
    meta = jnp.concatenate([place, route_weight, jnp.zeros((tok, 8 - 2 * TOP), jnp.float32)], axis=1).T
    cuts = ((0, Y_FIRST), (Y_FIRST, Z_PART), (Y_FIRST + Z_PART, tok - Y_FIRST - Z_PART))
    an = cuts[0][1]
    vmem, hbm = pl.BlockSpec(memory_space=pltpu.VMEM), pl.BlockSpec(memory_space=pl.ANY)
    kind = normed.dtype
    slots, buffers = local_experts * SLOT, min(4, local_experts)
    dma = pltpu.SemaphoreType.DMA
    mixed = pl.pallas_call(
        functools.partial(layer_kernel, n_tp, cuts),
        out_shape=jax.ShapeDtypeStruct((tok, width), kind),
        in_specs=[vmem, vmem, hbm, hbm, hbm],
        out_specs=vmem,
        scratch_shapes=[
            pltpu.VMEM((4, n_tp, tok, width), kind),
            pltpu.VMEM((4, n_tp) + meta.shape, jnp.float32),
            pltpu.VMEM((4, n_tp, slots, tok), kind),
            pltpu.VMEM((local_experts, 4 * n_tp * SLOT, 128), jnp.float32),
            pltpu.VMEM((local_experts, 4 * n_tp * SLOT, width), kind),
            pltpu.VMEM((buffers, width, hidden), kind),
            pltpu.VMEM((buffers, width, hidden), kind),
            pltpu.VMEM((buffers, hidden, width), kind),
            pltpu.VMEM((2, n_tp, tok, width), kind),
            pltpu.VMEM((2, n_tp, tok, width), kind),
            pltpu.VMEM((2, n_tp + 1, an, width), kind),
            pltpu.VMEM((n_tp + 1, tok, width), kind),
            pltpu.VMEM((an, width), kind),
            pltpu.VMEM((n_tp, tok, width), kind),
            dma((4, n_tp, 3, 4)),
            dma((4, n_tp, 3)),
            dma((4 * n_tp - 1,)),
            dma((4 * n_tp - 1,)),
            dma((3, buffers)),
            dma((2, n_tp)),
            dma((2, n_tp)),
            dma((2, n_tp)),
            dma((2, n_tp + 1)),
            dma((3, n_tp)),
            dma((3, n_tp + 1)),
            dma((3, n_tp)),
            dma((3, n_tp)),
            dma((2, max(2, n_tp))),
        ],
        compiler_params=pltpu.CompilerParams(
            collective_id=0, has_side_effects=True, vmem_limit_bytes=56 * 2**20
        ),
        name="routed_experts",
    )(normed, meta, w_gate, w_up, w_down)
    return mixed.astype(jnp.float32)


def per_device(
    resid_in,
    pool_input,
    pool_weight,
    pool_scale,
    out_weight,
    mix_gain,
    ffn_gain,
    w_gate,
    w_up,
    w_down,
    routes,
    route_weight,
    post_gain,
):
    n_sp = lax.axis_size("sp")
    n_tp = lax.axis_size("tp")
    seg_rows, channels = pool_input.shape
    if n_sp == 4 and n_tp == GROUPS and channels == GROUP_DIM and seg_rows == n_tp * 128:
        pooled = mixed_tokens(pool_input, pool_weight, pool_scale, n_tp)
    else:
        pooled = routed_pool(pool_input, pool_weight, pool_scale)
    tok_rows = pooled.shape[0]
    mix_out = jnp.dot(pooled, out_weight, preferred_element_type=jnp.float32)
    residual = (resid_in.astype(jnp.float32) + rms_scale(mix_out, mix_gain)).astype(jnp.bfloat16)
    normed = rms_scale(residual.astype(jnp.float32), ffn_gain).astype(jnp.bfloat16)
    width = normed.shape[1]
    if n_sp == 4 and n_tp <= 4 and tok_rows == 128 and w_gate.shape[2] <= 256 and w_gate.shape[0] <= 8 and tok_rows * width <= 128 * 2048:
        expert_mix = dense_experts(normed, routes, route_weight, w_gate, w_up, w_down)
        return (residual.astype(jnp.float32) + rms_scale(expert_mix, post_gain)).astype(jnp.bfloat16)
    local_experts = w_gate.shape[0]
    n_experts = local_experts * n_sp
    slot_total = n_experts * CAP
    flat_route = routes.reshape(-1)
    onehot = (flat_route[:, None] == lax.iota(jnp.int32, n_experts)[None, :]).astype(jnp.int32)
    slot_rank = jnp.sum((jnp.cumsum(onehot, axis=0) - onehot) * onehot, axis=1)
    slot_index = flat_route * CAP + slot_rank
    picker = slot_index[:, None] == lax.iota(jnp.int32, slot_total)[None, :]
    picker_rows = picker.astype(jnp.bfloat16)
    token_pick = jnp.sum(
        picker.reshape(tok_rows, TOP, slot_total).astype(jnp.float32), axis=1
    ).astype(jnp.bfloat16)
    buffer = lax.dot_general(
        token_pick, normed, (((0,), (0,)), ((), ())), preferred_element_type=jnp.float32
    )
    outgoing = buffer.astype(jnp.bfloat16).reshape(n_sp, local_experts * CAP, width)
    at_owner = lax.all_to_all(outgoing, "sp", split_axis=0, concat_axis=0, tiled=True)
    arrived = lax.all_gather(at_owner[:, None], "tp", axis=1, tiled=True)
    arrived = arrived.reshape(n_sp, n_tp, local_experts, CAP, width)
    gate_pre = jnp.einsum("sklcd,ldf->sklcf", arrived, w_gate, preferred_element_type=jnp.float32)
    upward = jnp.einsum("sklcd,ldf->sklcf", arrived, w_up, preferred_element_type=jnp.float32)
    activated = clamped_unit(gate_pre, upward).astype(jnp.bfloat16)
    terms = jnp.einsum("sklcf,lfd->kslcd", activated, w_down, preferred_element_type=jnp.float32)
    summed = lax.psum_scatter(
        terms.reshape(1 * lax.axis_size("tp"), n_sp, local_experts * CAP, width).astype(
            jnp.bfloat16
        ),
        "tp",
        scatter_dimension=0,
        tiled=True,
    ).astype(jnp.float32)
    results = summed[0].astype(jnp.bfloat16)
    returned = lax.all_to_all(results, "sp", split_axis=0, concat_axis=0, tiled=True).reshape(
        slot_total, width
    )
    gathered = jnp.dot(picker_rows, returned, preferred_element_type=jnp.float32)
    expert_mix = jnp.sum(gathered.reshape(tok_rows, TOP, width) * route_weight[:, :, None], axis=1)
    return (residual.astype(jnp.float32) + rms_scale(expert_mix, post_gain)).astype(jnp.bfloat16)


def solution(mesh):
    in_specs = (
        P(("grp", "sp", "tp"), None),
        P(("grp", "sp"), "tp"),
        P(),
        P(),
        P(),
        P(),
        P(),
        P("sp", None, "tp"),
        P("sp", None, "tp"),
        P("sp", "tp", None),
        P(("grp", "sp", "tp"), None),
        P(("grp", "sp", "tp"), None),
        P(),
    )
    out_specs = P(("grp", "sp", "tp"), None)
    return jax.shard_map(
        per_device, mesh=mesh, in_specs=in_specs, out_specs=out_specs, check_vma=False
    )
```
